256 devices in a mesh: grp: 2 (over z), sp: 64 (over y, x), tp: 2 (over core).
Axes of the slice: x: 8, y: 8, z: 2, core: 2. Of those that a mesh axis runs over, the one named last changes fastest.
The devices are a block of a 8x8x16 slice.
Arguments:
- probe_preactivation: bfloat16 [32768, 2048], P(('grp', 'sp'), 'tp'), parts along dimension 0, may hold values from -6 to 6
- retention_preactivation: bfloat16 [32768, 2048], P(('grp', 'sp'), 'tp'), parts along dimension 0, may hold values from -5 to 5.5
- source_entries: bfloat16 [32768, 2048], P(('grp', 'sp'), 'tp'), parts along dimension 0, may hold values from -6 to 6
- extra_log_retention: float32 [32768, 16], P(('grp', 'sp'), 'tp'), parts along dimension 0, may hold values from -1.39 to 0
- retention_slack: float32 [2048], P('tp'), as said below
- group_normalizer_gain: float32 [128], replicated, may hold values from 0.1 to 1.9
- readout_mapping_matrix: bfloat16 [2048, 2048], P('tp'), may hold values from -0.125 to 0.125
Outputs:
- mixed: bfloat16 [32768, 2048], P(('grp', 'sp', 'tp')), parts along dimension 0
The draws below stay inside these ranges and needn't reach their ends.
There are 2 independent parts, one for each index of `grp`. The reference program is written for one: setup_inputs(seed, part) draws one part's arguments, and reference() takes and returns one part's arrays. A program takes and returns all parts, laid end to end along the dimension named above; an argument that names none is the same for every part. Nothing has to cross between parts.
Inputs may be any that keep to these rules, and one draw needn't show every extreme that they name: `retention_slack`: every entry is positive.
All inputs are finite; a program needn't handle non-finite values.
Results may differ from the reference program's by a relative error of at most 0.014.
Values may be sent and summed in bfloat16 or wider, within the bound.
No kernel may reach another device: no remote copies, remote signals or barrier semaphores. Data moves between devices by JAX's collectives and lax.ppermute only.
A program may use at most 128 MiB of HBM per device.

```python
import math
import jax
import jax.numpy as jnp
from jax import lax

D = 2048
RECURRENT_HEADS = 16
HEAD = 128
SPAN = 128
TOK_DEV = 256
CHANNELS = 2048
SEQ = 16384
TOTAL_TOKENS = 16384


def draw_retention_preactivation(key, part):
    primary_random_key, secondary_random_key = jax.random.split(jax.random.fold_in(key, 11))
    baseline = jnp.clip(jax.random.normal(primary_random_key, (TOTAL_TOKENS, CHANNELS), jnp.float32), -4.0, 4.0)
    block_len = TOK_DEV // 2
    shifts = jax.random.uniform(secondary_random_key, (TOTAL_TOKENS // block_len, 1), jnp.float32, -1.0, 1.5)
    shifts = jnp.repeat(shifts, block_len, axis=0)
    return (baseline + shifts).astype(jnp.bfloat16)


def draw_retention_slack(key, part):
    primary_random_key, secondary_random_key, third_key = jax.random.split(jax.random.fold_in(key, 23), 3)
    shuffled = jax.random.permutation(primary_random_key, RECURRENT_HEADS)
    fast_count = RECURRENT_HEADS // 2
    low_end = math.log(0.04)
    high_end = math.log(0.07)
    fast_head = jnp.repeat(shuffled < fast_count, HEAD)
    quick_room = jnp.exp(jax.random.uniform(secondary_random_key, (CHANNELS,), jnp.float32, low_end, high_end))
    slow_room = jnp.exp(jax.random.uniform(third_key, (CHANNELS,), jnp.float32, math.log(0.2), 0.0)) / SEQ
    return jnp.where(fast_head, quick_room, slow_room).astype(jnp.float32)


def draw_extra_log_retention(key, part):
    primary_random_key, secondary_random_key = jax.random.split(jax.random.fold_in(key, 37))
    segment_rows = jax.random.randint(primary_random_key, (2, RECURRENT_HEADS), 0, TOTAL_TOKENS)
    segment_length = jax.random.uniform(secondary_random_key, (2, RECURRENT_HEADS), jnp.float32, math.log(0.5), math.log(0.8))
    token_positions = jnp.arange(TOTAL_TOKENS, dtype=jnp.int32)[:, None]
    final_output = jnp.where(token_positions == segment_rows[0][None], segment_length[0][None], 0.0)
    final_output = final_output + jnp.where(token_positions == segment_rows[1][None], segment_length[1][None], 0.0)
    return final_output.astype(jnp.float32)


def steps_of(rng, extent, shards, low, high):
    factor_of = 1.0
    for dim, blocks in shards:
        heights = jax.random.uniform(jax.random.fold_in(jax.random.fold_in(rng, 6), dim), (blocks,), jnp.float32, low / len(shards), high / len(shards))
        factor_of = factor_of * jnp.repeat(jnp.exp(heights), extent[dim] // blocks).reshape((-1,) + (1,) * (len(extent) - 1 - dim))
    return factor_of


def noise(rng, dims, deviation, reach, shards=(), kind=jnp.bfloat16):
    values = deviation * jax.random.normal(rng, dims, jnp.float32)
    if shards:
        values = values * steps_of(rng, dims, shards, -0.22, 0.18)
    return jnp.clip(values, -reach, reach).astype(kind)


def setup_inputs(seed: int = 0, part: int = 0) -> dict:
    streams_of = jax.random.split(jax.random.key(seed), 8)
    own_keys = jax.random.split(jax.random.fold_in(streams_of[7], part), 8)
    probe_preactivation = noise(own_keys[0], (TOTAL_TOKENS, CHANNELS), 1.0, 6.0, ((0, 64), (1, 2)))
    retention_preactivation = draw_retention_preactivation(jax.random.fold_in(jax.random.fold_in(streams_of[7], part), 71), part)
    source_entries = noise(own_keys[2], (TOTAL_TOKENS, CHANNELS), 1.0, 6.0, ((0, 64), (1, 2)))
    extra_log_retention = draw_extra_log_retention(jax.random.fold_in(jax.random.fold_in(streams_of[7], part), 71), part)
    retention_slack = draw_retention_slack(jax.random.fold_in(streams_of[7], 71), part)
    group_normalizer_gain = jnp.clip(1.0 + 0.18 * jax.random.normal(streams_of[5], (HEAD,), jnp.float32), 0.1, 1.9)
    readout_mapping_matrix = noise(streams_of[6], (CHANNELS, D), CHANNELS ** -0.5, 0.125, ((0, 2),))
    return {"probe_preactivation": probe_preactivation, "retention_preactivation": retention_preactivation, "source_entries": source_entries, "extra_log_retention": extra_log_retention, "retention_slack": retention_slack, "group_normalizer_gain": group_normalizer_gain, "readout_mapping_matrix": readout_mapping_matrix}


TOP_PRECISION = lax.Precision.HIGHEST

def rounded_values(value):
    return lax.optimization_barrier(value.astype(jnp.bfloat16)).astype(jnp.float32)

def assemble_arguments(probe_preactivation, retention_preactivation, source_entries, extra_log_retention, retention_slack):
    tokens_here = probe_preactivation.shape[0]
    group_count = extra_log_retention.shape[1]
    head_dim = probe_preactivation.shape[1] // group_count
    probe_matrix = jax.nn.silu(probe_preactivation.astype(jnp.float32)).reshape(tokens_here, group_count, head_dim)
    scaled_address_matrix = (retention_slack * jax.nn.sigmoid(-retention_preactivation.astype(jnp.float32))).reshape(tokens_here, group_count, head_dim)
    log_retention_factor = jnp.log1p(-scaled_address_matrix) + extra_log_retention[:, :, None]
    content_matrix = source_entries.astype(jnp.float32).reshape(tokens_here, group_count, head_dim)
    return (probe_matrix, scaled_address_matrix, content_matrix, log_retention_factor)

def block_pass(carried_state, pieces):
    probe_matrix, scaled_address_matrix, content_matrix, log_retention_factor = pieces
    span_len = probe_matrix.shape[0]
    running = jnp.cumsum(log_retention_factor, axis=0)
    raised_values = rounded_values(probe_matrix * jnp.exp(running))
    lowered = rounded_values(scaled_address_matrix * jnp.exp(-running))
    scores = jnp.einsum('thk,shk->hts', raised_values, lowered, precision=TOP_PRECISION)
    row_index = lax.broadcasted_iota(jnp.int32, (span_len, span_len), 0)
    col_index = lax.broadcasted_iota(jnp.int32, (span_len, span_len), 1)
    scores = rounded_values(jnp.where((row_index >= col_index)[None], scores, jnp.zeros_like(scores)))
    final_output = jnp.einsum('hts,shv->thv', scores, content_matrix, precision=TOP_PRECISION)
    final_output = final_output + jnp.einsum('csq,sqd->csd', raised_values, rounded_values(carried_state), precision=TOP_PRECISION)
    final_running_sum = running[-1]
    passed_state = rounded_values(scaled_address_matrix * jnp.exp(final_running_sum[None] - running))
    carried_state = jnp.exp(final_running_sum)[:, :, None] * carried_state + jnp.einsum('wcf,wcz->cfz', passed_state, content_matrix, precision=TOP_PRECISION)
    return (carried_state, final_output)

def finish(mixer_out, group_normalizer_gain):
    scale = lax.rsqrt(lax.optimization_barrier(jnp.mean(mixer_out * mixer_out, axis=-1, keepdims=True)) + 1e-06)
    normed = (mixer_out * scale * group_normalizer_gain).astype(jnp.bfloat16)
    return normed.reshape(mixer_out.shape[0], mixer_out.shape[1] * mixer_out.shape[2])

def reference(probe_preactivation, retention_preactivation, source_entries, extra_log_retention, retention_slack, group_normalizer_gain, readout_mapping_matrix):
    probe_matrix, scaled_address_matrix, content_matrix, log_retention_factor = assemble_arguments(probe_preactivation, retention_preactivation, source_entries, extra_log_retention, retention_slack)
    length = probe_matrix.shape[0]
    blocks = length // SPAN
    pieces = tuple((a.reshape(blocks, SPAN, RECURRENT_HEADS, HEAD) for a in (probe_matrix, scaled_address_matrix, content_matrix, log_retention_factor)))
    initial = jnp.zeros((RECURRENT_HEADS, HEAD, HEAD), jnp.float32)
    _, mixer_out = lax.scan(block_pass, initial, pieces)
    normed = finish(mixer_out.reshape(length, RECURRENT_HEADS, HEAD), group_normalizer_gain)
    return jnp.dot(normed, readout_mapping_matrix, preferred_element_type=jnp.float32).astype(jnp.bfloat16)
```

```python
import functools

import jax
import jax.numpy as jnp
from jax import lax
from jax.experimental import pallas as pl
from jax.experimental.pallas import tpu as pltpu
from jax.sharding import Mesh
from jax.sharding import PartitionSpec as P

SPAN = 128
HEAD = 128
SP = ("sp_0", "sp_1")
GRP_SP = ("grp", "sp_0", "sp_1")
GRP_SP_TP = ("grp", "sp_0", "sp_1", "tp")
F32 = jnp.float32
BF16 = jnp.bfloat16


def dot(a, b, contract):
    return lax.dot_general(a, b, (contract, ((), ())), preferred_element_type=F32)


def three_parts(x):
    high = x.astype(BF16)
    rest = x - high.astype(F32)
    middle = rest.astype(BF16)
    low = (rest - middle.astype(F32)).astype(BF16)
    return high, middle, low


def summed_rows(selection, x):
    return sum(dot(selection, part, ((1,), (0,))) for part in three_parts(x))


def keyed_and_log_decay(retention, slack, extra):
    keyed = slack * jax.nn.sigmoid(-retention.astype(F32))
    return keyed, jnp.log1p(-keyed) + extra


def ones_where(shape, compare):
    rows = lax.broadcasted_iota(jnp.int32, shape, 0)
    columns = lax.broadcasted_iota(jnp.int32, shape, 1)
    return compare(rows, columns)


def state_kernel(slabs, retention, source, extra, slack, message):
    tokens, channels = retention.shape
    later = ones_where((tokens, tokens), lambda r, c: c > r).astype(BF16)
    rows = HEAD // slabs
    for h in range(channels // HEAD):
        lanes = slice(h * HEAD, (h + 1) * HEAD)
        keyed, log_decay = keyed_and_log_decay(
            retention[:, lanes], slack[:, lanes], extra[:, h : h + 1]
        )
        ahead = summed_rows(later, log_decay)
        sent = (keyed * jnp.exp(ahead)).astype(BF16)
        state = dot(sent, source[:, lanes], ((0,), (0,)))
        message[h * slabs : (h + 1) * slabs, :rows, :] = state.astype(BF16).reshape(
            slabs, rows, HEAD
        )
        total = ahead[:1] + log_decay[:1]
        parts = jnp.concatenate(three_parts(total) + (jnp.zeros((5, HEAD), BF16),), axis=0)
        message[h * slabs : (h + 1) * slabs, rows:, :] = jnp.broadcast_to(
            parts[None], (slabs, 8, HEAD)
        )


def scan_kernel(slab, message, entering, by_channel):
    positions, rows, _ = entering.shape
    parts = message[:, rows:, :].astype(F32)
    decay = jnp.exp(parts[:, 0] + parts[:, 1] + parts[:, 2])
    by_channel[...] = decay.T
    start = pl.multiple_of(slab[0] * rows, rows)
    mine = by_channel[pl.ds(start, rows), :]
    state = jnp.zeros((rows, HEAD), F32)
    for i in range(positions):
        entering[i] = state.astype(BF16)
        if i + 1 < positions:
            state = mine[:, i : i + 1] * state + message[i, :rows, :].astype(F32)


def local_kernel(probe, retention, source, extra, slack, inside, reading):
    tokens, channels = retention.shape
    upto = ones_where((SPAN, SPAN), lambda r, c: c <= r)
    upto_ones = upto.astype(BF16)
    for h in range(channels // HEAD):
        lanes = slice(h * HEAD, (h + 1) * HEAD)
        before, decayed = None, None
        for b in range(tokens // SPAN):
            span = slice(b * SPAN, (b + 1) * SPAN)
            keyed, log_decay = keyed_and_log_decay(
                retention[span, lanes], slack[:, lanes], extra[span, h : h + 1]
            )
            values = source[span, lanes]
            pre = probe[span, lanes].astype(F32)
            query = pre / (1.0 + jnp.exp(-pre))
            running = summed_rows(upto_ones, log_decay)
            last = running[SPAN - 1 :]
            raised = query * jnp.exp(running)
            lifted = raised.astype(BF16)
            lowered = (keyed * jnp.exp(-running)).astype(BF16)
            scores = dot(lifted, lowered, ((1,), (1,)))
            weights = jnp.where(upto, scores, 0.0).astype(BF16)
            out = dot(weights, values, ((1,), (0,)))
            if before is not None:
                out = out + dot(lifted, before.astype(BF16), ((1,), (0,)))
                reading[span, lanes] = (query * jnp.exp(running + decayed)).astype(BF16)
            else:
                reading[span, lanes] = lifted
            inside[span, lanes] = out
            if (b + 1) * SPAN < tokens:
                sent = (keyed * jnp.exp(last - running)).astype(BF16)
                added = dot(sent, values, ((0,), (0,)))
                if before is None:
                    before, decayed = added, last
                else:
                    before = jnp.exp(last).reshape(HEAD, 1) * before + added
                    decayed = decayed + last


def output_kernel(half, inside, reading, entering, gain, matrix, out, normed):
    tokens = out.shape[0]
    start = pl.multiple_of(half[0] * tokens, tokens)
    rows = pl.ds(start, tokens)
    for h in range(entering.shape[0]):
        lanes = slice(h * HEAD, (h + 1) * HEAD)
        mixer = inside[rows, lanes] + dot(reading[rows, lanes], entering[h], ((1,), (0,)))
        scale = lax.rsqrt(jnp.mean(mixer * mixer, axis=-1, keepdims=True) + 1e-06)
        normed[:, lanes] = (mixer * scale * gain[...]).astype(BF16)
    out[...] = dot(normed[...], matrix[...], ((1,), (0,))).astype(out.dtype)


def in_vmem(count):
    return [pl.BlockSpec(memory_space=pltpu.VMEM)] * count


SCALAR = pl.BlockSpec(memory_space=pltpu.SMEM)


def call(kernel, name, inputs, out_shape, flops, scratch=(), scalars=0):
    moved = sum(a.size * a.dtype.itemsize for a in inputs)
    multiple = isinstance(out_shape, (list, tuple))
    outs = out_shape if multiple else [out_shape]
    moved += sum(a.size * a.dtype.itemsize for a in outs)
    return pl.pallas_call(
        kernel,
        name=name,
        out_shape=out_shape,
        in_specs=[SCALAR] * scalars + in_vmem(len(inputs) - scalars),
        out_specs=in_vmem(len(outs)) if multiple else in_vmem(1)[0],
        scratch_shapes=scratch,
        compiler_params=pltpu.CompilerParams(vmem_limit_bytes=48 << 20),
        cost_estimate=pl.CostEstimate(flops=flops, bytes_accessed=moved, transcendentals=0),
    )(*inputs)


def body(
    probe_preactivation,
    retention_preactivation,
    source_entries,
    extra_log_retention,
    retention_slack,
    group_normalizer_gain,
    readout_mapping_matrix,
):
    tokens, channels = probe_preactivation.shape
    heads = channels // HEAD
    positions = lax.axis_size(SP)
    slabs = positions // heads
    rows = HEAD // slabs
    width = readout_mapping_matrix.shape[1]
    slack = retention_slack.reshape(1, channels)
    gain = group_normalizer_gain.reshape(1, HEAD)
    flops = 2 * tokens * channels * HEAD

    message = call(
        functools.partial(state_kernel, slabs),
        "state",
        (retention_preactivation, source_entries, extra_log_retention, slack),
        jax.ShapeDtypeStruct((positions, rows + 8, HEAD), BF16),
        4 * flops,
    )
    arrived = lax.all_to_all(message, SP, split_axis=0, concat_axis=0, tiled=True)
    inside, reading = call(
        local_kernel,
        "local",
        (
            probe_preactivation,
            retention_preactivation,
            source_entries,
            extra_log_retention,
            slack,
        ),
        [
            jax.ShapeDtypeStruct((tokens, channels), F32),
            jax.ShapeDtypeStruct((tokens, channels), BF16),
        ],
        6 * flops,
    )
    slab = (lax.axis_index(SP) % slabs).astype(jnp.int32).reshape(1)
    scanned = call(
        scan_kernel,
        "scan",
        (slab, arrived),
        jax.ShapeDtypeStruct((positions, rows, HEAD), BF16),
        flops,
        scratch=[pltpu.VMEM((HEAD, positions), F32)],
        scalars=1,
    )
    entering = lax.all_to_all(scanned, SP, split_axis=0, concat_axis=0, tiled=True)
    entering = entering.reshape(heads, HEAD, HEAD)

    mine = lax.axis_index("tp").astype(jnp.int32)
    half = tokens // lax.axis_size("tp")

    def projected(which, dtype):
        return call(
            output_kernel,
            "output",
            (which.reshape(1), inside, reading, entering, gain, readout_mapping_matrix),
            jax.ShapeDtypeStruct((half, width), dtype),
            half * channels * width * 2,
            scratch=[pltpu.VMEM((half, channels), BF16)],
            scalars=1,
        )

    away = projected(1 - mine, BF16)
    received = lax.ppermute(away, "tp", [(0, 1), (1, 0)])
    kept = projected(mine, F32)
    return (kept + received.astype(F32)).astype(BF16)


def solution(mesh):
    finer = Mesh(
        mesh.devices.reshape(mesh.shape["grp"], 8, 8, mesh.shape["tp"]),
        ("grp", "sp_0", "sp_1", "tp"),
    )
    in_specs = (
        P(GRP_SP, "tp"),
        P(GRP_SP, "tp"),
        P(GRP_SP, "tp"),
        P(GRP_SP, "tp"),
        P("tp"),
        P(),
        P("tp", None),
    )
    out_specs = P(GRP_SP_TP, None)
    return jax.shard_map(body, mesh=finer, in_specs=in_specs, out_specs=out_specs, check_vma=False)
```

```python
import functools

import jax
import jax.numpy as jnp
from jax import lax
from jax.experimental import pallas as pl
from jax.experimental.pallas import tpu as pltpu
from jax.sharding import Mesh
from jax.sharding import PartitionSpec as P

SPAN = 128
HEAD = 128
SP = ("sp_0", "sp_1")
GRP_SP = ("grp", "sp_0", "sp_1")
GRP_SP_TP = ("grp", "sp_0", "sp_1", "tp")
F32 = jnp.float32
BF16 = jnp.bfloat16


def dot(a, b, contract):
    return lax.dot_general(a, b, (contract, ((), ())), preferred_element_type=F32)


def two_parts(x):
    high = x.astype(BF16)
    return high, (x - high.astype(F32)).astype(BF16)


def summed_rows(selection, x):
    return sum(dot(selection, part, ((1,), (0,))) for part in two_parts(x))


def keyed_and_log_decay(retention, slack, extra):
    keyed = slack * jax.nn.sigmoid(-retention.astype(F32))
    return keyed, jnp.log1p(-keyed) + extra


def rows_and_columns(shape):
    return lax.broadcasted_iota(jnp.int32, shape, 0), lax.broadcasted_iota(jnp.int32, shape, 1)


def state_kernel(
    slabs, retention, source, far_extra, far_slack, message, r_in, v_in, extra, slack, sems, small
):
    tokens, channels = retention.shape
    wide = 2 * HEAD
    pairs = channels // wide
    first = [
        pltpu.make_async_copy(a, b, small.at[i])
        for i, (a, b) in enumerate(((far_extra, extra), (far_slack, slack)))
    ]
    for copy in first:
        copy.start()

    def copies(source_ref, target, row):
        return [
            pltpu.make_async_copy(
                source_ref.at[:, p * wide : (p + 1) * wide], target.at[p], sems.at[row, p]
            )
            for p in range(pairs)
        ]

    r_copies, v_copies = (copies(retention, r_in, 0), copies(source, v_in, 1))
    for p in range(pairs):
        r_copies[p].start()
        v_copies[p].start()
    r, c = rows_and_columns((tokens, tokens))
    later = (c > r).astype(BF16)
    rows = HEAD // slabs
    for copy in first:
        copy.wait()
    by_token = extra[...].T
    for p in range(pairs):
        r_copies[p].wait()
        added = jnp.concatenate(
            [
                jnp.broadcast_to(by_token[:, h : h + 1], (tokens, HEAD))
                for h in (2 * p, 2 * p + 1)
            ],
            axis=1,
        )
        keyed, log_decay = keyed_and_log_decay(
            r_in[p], slack[:, p * wide : (p + 1) * wide], added
        )
        ahead = summed_rows(later, log_decay)
        sent = (keyed * jnp.exp(ahead)).astype(BF16)
        total = ahead[:1] + log_decay[:1]
        parts = jnp.concatenate(two_parts(total) + (jnp.zeros((6, wide), BF16),), axis=0)
        v_copies[p].wait()
        for k in range(2):
            lanes = slice(k * HEAD, (k + 1) * HEAD)
            h = 2 * p + k
            state = dot(sent[:, lanes], v_in[p, :, lanes], ((0,), (0,)))
            message[h * slabs : (h + 1) * slabs, :rows, :] = state.astype(BF16).reshape(
                slabs, rows, HEAD
            )
            message[h * slabs : (h + 1) * slabs, rows:, :] = jnp.broadcast_to(
                parts[None, :, lanes], (slabs, 8, HEAD)
            )


def scan_kernel(slabs, message, entering, by_channel):
    positions, rows, _ = entering.shape
    slab = lax.rem(lax.axis_index(SP), slabs)
    parts = message[:, rows:, :].astype(F32)
    by_channel[...] = jnp.exp(parts[:, 0] + parts[:, 1]).T
    mine = by_channel[pl.ds(pl.multiple_of(slab * rows, rows), rows), :]
    state = jnp.zeros((rows, HEAD), F32)
    for i in range(positions):
        entering[i] = state.astype(BF16)
        if i + 1 < positions:
            state = mine[:, i : i + 1] * state + message[i, :rows, :].astype(F32)


def local_kernel(probe, retention, source, extra, slack, inside, reading):
    tokens, channels = retention.shape
    r, c = rows_and_columns((SPAN, SPAN))
    upto = c <= r
    upto_ones = upto.astype(BF16)
    by_token = extra[...].T
    for h in range(channels // HEAD):
        lanes = slice(h * HEAD, (h + 1) * HEAD)
        before, decayed = None, None
        for b in range(tokens // SPAN):
            span = slice(b * SPAN, (b + 1) * SPAN)
            keyed, log_decay = keyed_and_log_decay(
                retention[span, lanes], slack[:, lanes], by_token[span, h : h + 1]
            )
            values = source[span, lanes]
            query = jax.nn.silu(probe[span, lanes].astype(F32))
            running = summed_rows(upto_ones, log_decay)
            last = running[SPAN - 1 :]
            raised = query * jnp.exp(running)
            lifted = raised.astype(BF16)
            lowered = (keyed * jnp.exp(-running)).astype(BF16)
            scores = dot(lifted, lowered, ((1,), (1,)))
            weights = jnp.where(upto, scores, 0.0).astype(BF16)
            out = dot(weights, values, ((1,), (0,)))
            if before is not None:
                out = out + dot(lifted, before.astype(BF16), ((1,), (0,)))
                reading[span, lanes] = (query * jnp.exp(running + decayed)).astype(BF16)
            else:
                reading[span, lanes] = lifted
            inside[span, lanes] = out
            if (b + 1) * SPAN < tokens:
                sent = (keyed * jnp.exp(last - running)).astype(BF16)
                added = dot(sent, values, ((0,), (0,)))
                if before is None:
                    before, decayed = added, last
                else:
                    before = jnp.exp(last).reshape(HEAD, 1) * before + added
                    decayed = decayed + last


def output_kernel(away, far, inside, reading, entering, gain, out, normed, matrix, sems):
    tokens, width = out.shape
    pieces = matrix.shape[0]
    wide = width // pieces
    copies = [
        pltpu.make_async_copy(far.at[:, i * wide : (i + 1) * wide], matrix.at[i], sems.at[i])
        for i in range(pieces)
    ]
    for copy in copies:
        copy.start()
    mine = lax.axis_index("tp")
    half = 1 - mine if away else mine
    rows = pl.ds(pl.multiple_of(half * tokens, tokens), tokens)
    for h in range(entering.shape[0]):
        lanes = slice(h * HEAD, (h + 1) * HEAD)
        mixer = inside[rows, lanes] + dot(reading[rows, lanes], entering[h], ((1,), (0,)))
        scale = lax.rsqrt(jnp.mean(mixer * mixer, axis=-1, keepdims=True) + 1e-06)
        normed[:, lanes] = (mixer * scale * gain[...]).astype(BF16)
    for i, copy in enumerate(copies):
        copy.wait()
        out[:, i * wide : (i + 1) * wide] = dot(normed[...], matrix[i], ((1,), (0,))).astype(
            out.dtype
        )


VMEM = 67043328
IN_VMEM = pl.BlockSpec(memory_space=pltpu.VMEM)
IN_HBM = pl.BlockSpec(memory_space=pltpu.HBM)


def call(kernel, name, far, near, outs, flops, scratch=(), left=24 << 20):
    inputs = (*far, *near)
    moved = sum(a.size * a.dtype.itemsize for a in (*inputs, *outs))
    results = pl.pallas_call(
        kernel,
        name=name,
        out_shape=outs,
        in_specs=[IN_HBM] * len(far) + [IN_VMEM] * len(near),
        out_specs=[IN_VMEM] * len(outs),
        scratch_shapes=scratch,
        compiler_params=pltpu.CompilerParams(vmem_limit_bytes=VMEM - left),
        cost_estimate=pl.CostEstimate(flops=flops, bytes_accessed=moved, transcendentals=0),
    )(*inputs)
    return results if len(outs) > 1 else results[0]


def body(
    probe_preactivation,
    retention_preactivation,
    source_entries,
    extra_log_retention,
    retention_slack,
    group_normalizer_gain,
    readout_mapping_matrix,
):
    tokens, channels = probe_preactivation.shape
    heads = channels // HEAD
    positions = lax.axis_size(SP)
    slabs = positions // heads
    rows = HEAD // slabs
    width = readout_mapping_matrix.shape[1]
    slack = retention_slack.reshape(1, channels)
    gain = group_normalizer_gain.reshape(1, HEAD)
    extra = extra_log_retention.T
    flops = 2 * tokens * channels * HEAD
    pairs = channels // (2 * HEAD)

    message = call(
        functools.partial(state_kernel, slabs),
        "state",
        (retention_preactivation, source_entries, extra, slack),
        (),
        [jax.ShapeDtypeStruct((positions, rows + 8, HEAD), BF16)],
        4 * flops,
        [pltpu.VMEM((pairs, tokens, 2 * HEAD), BF16)] * 2
        + [pltpu.VMEM(extra.shape, F32), pltpu.VMEM(slack.shape, F32)]
        + [pltpu.SemaphoreType.DMA((2, pairs)), pltpu.SemaphoreType.DMA((2,))],
        21 << 19,
    )
    arrived = lax.all_to_all(message, SP, split_axis=0, concat_axis=0, tiled=True)
    inside, reading = call(
        local_kernel,
        "local",
        (),
        (probe_preactivation, retention_preactivation, source_entries, extra, slack),
        [
            jax.ShapeDtypeStruct((tokens, channels), F32),
            jax.ShapeDtypeStruct((tokens, channels), BF16),
        ],
        6 * flops,
    )
    scanned = call(
        functools.partial(scan_kernel, slabs),
        "scan",
        (),
        (arrived,),
        [jax.ShapeDtypeStruct((positions, rows, HEAD), BF16)],
        flops,
        [pltpu.VMEM((HEAD, positions), F32)],
    )
    entering = lax.all_to_all(scanned, SP, split_axis=0, concat_axis=0, tiled=True)
    entering = entering.reshape(heads, HEAD, HEAD)
    half = tokens // lax.axis_size("tp")

    pieces = 4

    def projected(away, dtype):
        return call(
            functools.partial(output_kernel, away),
            "away" if away else "kept",
            (readout_mapping_matrix,),
            (inside, reading, entering, gain),
            [jax.ShapeDtypeStruct((half, width), dtype)],
            half * channels * width * 2,
            [
                pltpu.VMEM((half, channels), BF16),
                pltpu.VMEM((pieces, channels, width // pieces), BF16),
                pltpu.SemaphoreType.DMA((pieces,)),
            ],
            14 << 20,
        )

    received = lax.ppermute(projected(True, BF16), "tp", [(0, 1), (1, 0)])
    return (projected(False, F32) + received.astype(F32)).astype(BF16)


def solution(mesh):
    finer = Mesh(
        mesh.devices.reshape(mesh.shape["grp"], 8, 8, mesh.shape["tp"]),
        ("grp", "sp_0", "sp_1", "tp"),
    )
    in_specs = (
        P(GRP_SP, "tp"),
        P(GRP_SP, "tp"),
        P(GRP_SP, "tp"),
        P(GRP_SP, "tp"),
        P("tp"),
        P(),
        P("tp", None),
    )
    out_specs = P(GRP_SP_TP, None)
    return jax.shard_map(body, mesh=finer, in_specs=in_specs, out_specs=out_specs, check_vma=False)
```

```python
import functools

import jax
import jax.numpy as jnp
from jax import lax
from jax.experimental import pallas as pl
from jax.experimental.pallas import tpu as pltpu
from jax.sharding import Mesh
from jax.sharding import PartitionSpec as P

SPAN = 128
HEAD = 128
SP = ("sp_0", "sp_1")
GRP_SP = ("grp", "sp_0", "sp_1")
GRP_SP_TP = ("grp", "sp_0", "sp_1", "tp")
SWAP = ((0, 1), (1, 0))
F32 = jnp.float32
BF16 = jnp.bfloat16


def dot(a, b, contract):
    return lax.dot_general(a, b, (contract, ((), ())), preferred_element_type=F32)


def two_parts(x):
    high = x.astype(BF16)
    return high, (x - high.astype(F32)).astype(BF16)


def summed_rows(selection, x):
    return sum(dot(selection, part, ((1,), (0,))) for part in two_parts(x))


def keyed_and_log_decay(retention, slack, extra):
    keyed = slack * jax.nn.sigmoid(-retention.astype(F32))
    return keyed, jnp.log1p(-keyed) + extra


def rows_and_columns(shape):
    return lax.broadcasted_iota(jnp.int32, shape, 0), lax.broadcasted_iota(jnp.int32, shape, 1)


def state_kernel(
    slabs, retention, source, far_extra, far_slack, message, r_in, v_in, extra, slack, sems, small
):
    tokens, channels = retention.shape
    wide = 2 * HEAD
    pairs = channels // wide
    first = [
        pltpu.make_async_copy(a, b, small.at[i])
        for i, (a, b) in enumerate(((far_extra, extra), (far_slack, slack)))
    ]
    for copy in first:
        copy.start()

    def copies(source_ref, target, row):
        return [
            pltpu.make_async_copy(
                source_ref.at[:, p * wide : (p + 1) * wide], target.at[p], sems.at[row, p]
            )
            for p in range(pairs)
        ]

    r_copies, v_copies = (copies(retention, r_in, 0), copies(source, v_in, 1))
    for p in range(pairs):
        r_copies[p].start()
        v_copies[p].start()
    r, c = rows_and_columns((tokens, tokens))
    later = (c > r).astype(BF16)
    rows = HEAD // slabs
    for copy in first:
        copy.wait()
    by_token = extra[...].T
    for p in range(pairs):
        r_copies[p].wait()
        added = jnp.concatenate(
            [
                jnp.broadcast_to(by_token[:, h : h + 1], (tokens, HEAD))
                for h in (2 * p, 2 * p + 1)
            ],
            axis=1,
        )
        keyed, log_decay = keyed_and_log_decay(
            r_in[p], slack[:, p * wide : (p + 1) * wide], added
        )
        ahead = summed_rows(later, log_decay)
        sent = (keyed * jnp.exp(ahead)).astype(BF16)
        total = ahead[:1] + log_decay[:1]
        parts = jnp.concatenate(two_parts(total) + (jnp.zeros((6, wide), BF16),), axis=0)
        v_copies[p].wait()
        for k in range(2):
            lanes = slice(k * HEAD, (k + 1) * HEAD)
            h = 2 * p + k
            state = dot(sent[:, lanes], v_in[p, :, lanes], ((0,), (0,)))
            message[h * slabs : (h + 1) * slabs, :rows, :] = state.astype(BF16).reshape(
                slabs, rows, HEAD
            )
            message[h * slabs : (h + 1) * slabs, rows:, :] = jnp.broadcast_to(
                parts[None, :, lanes], (slabs, 8, HEAD)
            )


def scan_kernel(slabs, message, entering, by_channel):
    positions, rows, _ = entering.shape
    slab = lax.rem(lax.axis_index(SP), slabs)
    parts = message[:, rows:, :].astype(F32)
    by_channel[...] = jnp.exp(parts[:, 0] + parts[:, 1]).T
    mine = by_channel[pl.ds(pl.multiple_of(slab * rows, rows), rows), :]
    state = jnp.zeros((rows, HEAD), F32)
    for i in range(positions):
        entering[i] = state.astype(BF16)
        if i + 1 < positions:
            state = mine[:, i : i + 1] * state + message[i, :rows, :].astype(F32)


def local_kernel(probe, retention, source, extra, slack, inside, reading):
    tokens, channels = retention.shape
    r, c = rows_and_columns((SPAN, SPAN))
    upto = c <= r
    upto_ones = upto.astype(BF16)
    by_token = extra[...].T
    for h in range(channels // HEAD):
        lanes = slice(h * HEAD, (h + 1) * HEAD)
        before, decayed = None, None
        for b in range(tokens // SPAN):
            span = slice(b * SPAN, (b + 1) * SPAN)
            keyed, log_decay = keyed_and_log_decay(
                retention[span, lanes], slack[:, lanes], by_token[span, h : h + 1]
            )
            values = source[span, lanes]
            query = jax.nn.silu(probe[span, lanes].astype(F32))
            running = summed_rows(upto_ones, log_decay)
            last = running[SPAN - 1 :]
            raised = query * jnp.exp(running)
            lifted = raised.astype(BF16)
            lowered = (keyed * jnp.exp(-running)).astype(BF16)
            scores = dot(lifted, lowered, ((1,), (1,)))
            weights = jnp.where(upto, scores, 0.0).astype(BF16)
            out = dot(weights, values, ((1,), (0,)))
            if before is not None:
                out = out + dot(lifted, before.astype(BF16), ((1,), (0,)))
                reading[span, lanes] = (query * jnp.exp(running + decayed)).astype(BF16)
            else:
                reading[span, lanes] = lifted
            inside[span, lanes] = out
            if (b + 1) * SPAN < tokens:
                sent = (keyed * jnp.exp(last - running)).astype(BF16)
                added = dot(sent, values, ((0,), (0,)))
                if before is None:
                    before, decayed = added, last
                else:
                    before = jnp.exp(last).reshape(HEAD, 1) * before + added
                    decayed = decayed + last


def norm_kernel(inside, reading, entering, gain, mine, other):
    tokens = mine.shape[0]
    index = lax.axis_index("tp")
    for half, out in ((1 - index, other), (index, mine)):
        rows = pl.ds(pl.multiple_of(half * tokens, tokens), tokens)
        for h in range(entering.shape[0]):
            lanes = slice(h * HEAD, (h + 1) * HEAD)
            mixer = inside[rows, lanes] + dot(reading[rows, lanes], entering[h], ((1,), (0,)))
            scale = lax.rsqrt(jnp.mean(mixer * mixer, axis=-1, keepdims=True) + 1e-06)
            out[:, lanes] = (mixer * scale * gain[...]).astype(BF16)


def own_kernel(far, mine, out, matrix, sems):
    pieces = matrix.shape[0]
    wide = out.shape[1] // pieces
    copies = [
        pltpu.make_async_copy(far.at[:, i * wide : (i + 1) * wide], matrix.at[i], sems.at[i])
        for i in range(pieces)
    ]
    for copy in copies:
        copy.start()
    for i, copy in enumerate(copies):
        copy.wait()
        out[:, i * wide : (i + 1) * wide] = dot(mine[...], matrix[i], ((1,), (0,)))


def final_kernel(own, received, matrix, far, out, sems):
    pieces = out.shape[0]
    wide = own.shape[1] // pieces
    copies = []
    for i in range(pieces):
        columns = slice(i * wide, (i + 1) * wide)
        added = dot(received[...], matrix[:, columns], ((1,), (0,)))
        out[i] = (own[:, columns] + added).astype(BF16)
        copies.append(pltpu.make_async_copy(out.at[i], far.at[:, columns], sems.at[i]))
        copies[-1].start()
    for copy in copies:
        copy.wait()


VMEM = 67043328
IN_VMEM = pl.BlockSpec(memory_space=pltpu.VMEM)
IN_HBM = pl.BlockSpec(memory_space=pltpu.HBM)


def call(kernel, name, far, near, outs, flops, scratch=(), left=24 << 20, out_spec=IN_VMEM):
    inputs = (*far, *near)
    moved = sum(a.size * a.dtype.itemsize for a in (*inputs, *outs))
    results = pl.pallas_call(
        kernel,
        name=name,
        out_shape=outs,
        in_specs=[IN_HBM] * len(far) + [IN_VMEM] * len(near),
        out_specs=[out_spec] * len(outs),
        scratch_shapes=scratch,
        compiler_params=pltpu.CompilerParams(vmem_limit_bytes=VMEM - left),
        cost_estimate=pl.CostEstimate(flops=flops, bytes_accessed=moved, transcendentals=0),
    )(*inputs)
    return results if len(outs) > 1 else results[0]


def body(
    probe_preactivation,
    retention_preactivation,
    source_entries,
    extra_log_retention,
    retention_slack,
    group_normalizer_gain,
    readout_mapping_matrix,
):
    tokens, channels = probe_preactivation.shape
    heads = channels // HEAD
    positions = lax.axis_size(SP)
    slabs = positions // heads
    rows = HEAD // slabs
    width = readout_mapping_matrix.shape[1]
    slack = retention_slack.reshape(1, channels)
    gain = group_normalizer_gain.reshape(1, HEAD)
    extra = extra_log_retention.T
    flops = 2 * tokens * channels * HEAD
    pairs = channels // (2 * HEAD)

    message = call(
        functools.partial(state_kernel, slabs),
        "state",
        (retention_preactivation, source_entries, extra, slack),
        (),
        [jax.ShapeDtypeStruct((positions, rows + 8, HEAD), BF16)],
        4 * flops,
        [pltpu.VMEM((pairs, tokens, 2 * HEAD), BF16)] * 2
        + [pltpu.VMEM(extra.shape, F32), pltpu.VMEM(slack.shape, F32)]
        + [pltpu.SemaphoreType.DMA((2, pairs)), pltpu.SemaphoreType.DMA((2,))],
        21 << 19,
    )
    arrived = lax.all_to_all(message, SP, split_axis=0, concat_axis=0, tiled=True)
    inside, reading = call(
        local_kernel,
        "local",
        (),
        (probe_preactivation, retention_preactivation, source_entries, extra, slack),
        [
            jax.ShapeDtypeStruct((tokens, channels), F32),
            jax.ShapeDtypeStruct((tokens, channels), BF16),
        ],
        6 * flops,
    )
    arrived, inside, reading, matrix = lax.optimization_barrier(
        (arrived, inside, reading, readout_mapping_matrix)
    )
    matrix = lax.ppermute(matrix, "tp", SWAP)
    scanned = call(
        functools.partial(scan_kernel, slabs),
        "scan",
        (),
        (arrived,),
        [jax.ShapeDtypeStruct((positions, rows, HEAD), BF16)],
        flops,
        [pltpu.VMEM((HEAD, positions), F32)],
    )
    entering = lax.all_to_all(scanned, SP, split_axis=0, concat_axis=0, tiled=True)
    entering = entering.reshape(heads, HEAD, HEAD)
    half = tokens // lax.axis_size("tp")

    projection = half * channels * width * 2
    mine, other = call(
        norm_kernel,
        "norm",
        (),
        (inside, reading, entering, gain),
        [jax.ShapeDtypeStruct((half, channels), BF16)] * 2,
        flops,
    )
    received = lax.ppermute(other, "tp", SWAP)
    pieces = 4
    own = call(
        own_kernel,
        "own",
        (readout_mapping_matrix,),
        (mine,),
        [jax.ShapeDtypeStruct((half, width), F32)],
        projection,
        [
            pltpu.VMEM((pieces, channels, width // pieces), BF16),
            pltpu.SemaphoreType.DMA((pieces,)),
        ],
        17 << 20,
    )
    return call(
        final_kernel,
        "final",
        (),
        (own, received, matrix),
        [jax.ShapeDtypeStruct((half, width), BF16)],
        projection,
        [pltpu.VMEM((pieces, half, width // pieces), BF16), pltpu.SemaphoreType.DMA((pieces,))],
        out_spec=IN_HBM,
    )


def solution(mesh):
    finer = Mesh(
        mesh.devices.reshape(mesh.shape["grp"], 8, 8, mesh.shape["tp"]),
        ("grp", "sp_0", "sp_1", "tp"),
    )
    in_specs = (
        P(GRP_SP, "tp"),
        P(GRP_SP, "tp"),
        P(GRP_SP, "tp"),
        P(GRP_SP, "tp"),
        P("tp"),
        P(),
        P("tp", None),
    )
    out_specs = P(GRP_SP_TP, None)
    return jax.shard_map(body, mesh=finer, in_specs=in_specs, out_specs=out_specs, check_vma=False)
```

```python
import functools

import jax
import jax.numpy as jnp
from jax import lax
from jax.experimental import pallas as pl
from jax.experimental.pallas import tpu as pltpu
from jax.sharding import Mesh
from jax.sharding import PartitionSpec as P

SPAN = 128
HEAD = 128
SP = ("sp_0", "sp_1")
GRP_SP = ("grp", "sp_0", "sp_1")
GRP_SP_TP = ("grp", "sp_0", "sp_1", "tp")
SWAP = ((0, 1), (1, 0))
STAY = ((0, 0), (1, 1))
F32 = jnp.float32
BF16 = jnp.bfloat16


def dot(a, b, contract):
    return lax.dot_general(a, b, (contract, ((), ())), preferred_element_type=F32)


def two_parts(x):
    high = x.astype(BF16)
    return high, (x - high.astype(F32)).astype(BF16)


def summed_rows(selection, x):
    return sum(dot(selection, part, ((1,), (0,))) for part in two_parts(x))


def keyed_and_log_decay(retention, slack, extra):
    keyed = slack * jax.nn.sigmoid(-retention.astype(F32))
    return keyed, jnp.log1p(-keyed) + extra


def rows_and_columns(shape):
    return lax.broadcasted_iota(jnp.int32, shape, 0), lax.broadcasted_iota(jnp.int32, shape, 1)


def state_kernel(slabs, retention, source, extra, slack, message):
    tokens, channels = retention.shape
    wide = 2 * HEAD
    r, c = rows_and_columns((tokens, tokens))
    later = (c > r).astype(BF16)
    rows = HEAD // slabs
    by_token = extra[...].T
    for p in range(channels // wide):
        lanes = slice(p * wide, (p + 1) * wide)
        added = jnp.concatenate(
            [
                jnp.broadcast_to(by_token[:, h : h + 1], (tokens, HEAD))
                for h in (2 * p, 2 * p + 1)
            ],
            axis=1,
        )
        keyed, log_decay = keyed_and_log_decay(
            retention[:, lanes], slack[:, lanes], added
        )
        ahead = summed_rows(later, log_decay)
        sent = (keyed * jnp.exp(ahead)).astype(BF16)
        total = ahead[:1] + log_decay[:1]
        parts = jnp.concatenate(two_parts(total) + (jnp.zeros((6, wide), BF16),), axis=0)
        for k in range(2):
            h = 2 * p + k
            part = slice(k * HEAD, (k + 1) * HEAD)
            values = source[:, h * HEAD : (h + 1) * HEAD]
            state = dot(sent[:, part], values, ((0,), (0,)))
            message[h * slabs : (h + 1) * slabs, :rows, :] = state.astype(BF16).reshape(
                slabs, rows, HEAD
            )
            message[h * slabs : (h + 1) * slabs, rows:, :] = jnp.broadcast_to(
                parts[None, :, part], (slabs, 8, HEAD)
            )


def scan_kernel(slabs, message, entering, by_channel):
    positions, rows, _ = entering.shape
    slab = lax.rem(lax.axis_index(SP), slabs)
    parts = message[:, rows:, :].astype(F32)
    by_channel[...] = jnp.exp(parts[:, 0] + parts[:, 1]).T
    mine = by_channel[pl.ds(pl.multiple_of(slab * rows, rows), rows), :]
    state = jnp.zeros((rows, HEAD), F32)
    for i in range(positions):
        entering[i] = state.astype(BF16)
        if i + 1 < positions:
            state = mine[:, i : i + 1] * state + message[i, :rows, :].astype(F32)


def local_kernel(probe, retention, source, extra, slack, inside, reading):
    tokens, channels = retention.shape
    r, c = rows_and_columns((SPAN, SPAN))
    upto = c <= r
    upto_ones = upto.astype(BF16)
    by_token = extra[...].T
    for h in range(channels // HEAD):
        lanes = slice(h * HEAD, (h + 1) * HEAD)
        before, decayed = None, None
        for b in range(tokens // SPAN):
            span = slice(b * SPAN, (b + 1) * SPAN)
            keyed, log_decay = keyed_and_log_decay(
                retention[span, lanes], slack[:, lanes], by_token[span, h : h + 1]
            )
            values = source[span, lanes]
            query = jax.nn.silu(probe[span, lanes].astype(F32))
            running = summed_rows(upto_ones, log_decay)
            last = running[SPAN - 1 :]
            raised = query * jnp.exp(running)
            lifted = raised.astype(BF16)
            lowered = (keyed * jnp.exp(-running)).astype(BF16)
            scores = dot(lifted, lowered, ((1,), (1,)))
            weights = jnp.where(upto, scores, 0.0).astype(BF16)
            out = dot(weights, values, ((1,), (0,)))
            if before is not None:
                out = out + dot(lifted, before.astype(BF16), ((1,), (0,)))
                reading[span, lanes] = (query * jnp.exp(running + decayed)).astype(BF16)
            else:
                reading[span, lanes] = lifted
            inside[span, lanes] = out
            if (b + 1) * SPAN < tokens:
                sent = (keyed * jnp.exp(last - running)).astype(BF16)
                added = dot(sent, values, ((0,), (0,)))
                if before is None:
                    before, decayed = added, last
                else:
                    before = jnp.exp(last).reshape(HEAD, 1) * before + added
                    decayed = decayed + last


def norm_kernel(inside, reading, entering, gain, mine, other):
    tokens = mine.shape[0]
    index = lax.axis_index("tp")
    for half, out in ((1 - index, other), (index, mine)):
        rows = pl.ds(pl.multiple_of(half * tokens, tokens), tokens)
        for h in range(entering.shape[0]):
            lanes = slice(h * HEAD, (h + 1) * HEAD)
            mixer = inside[rows, lanes] + dot(reading[rows, lanes], entering[h], ((1,), (0,)))
            scale = lax.rsqrt(jnp.mean(mixer * mixer, axis=-1, keepdims=True) + 1e-06)
            out[:, lanes] = (mixer * scale * gain[...]).astype(BF16)


def own_kernel(mine, matrix, out):
    out[...] = dot(mine[...], matrix[...], ((1,), (0,)))


def final_kernel(own, received, matrix, far, out, sems):
    pieces = out.shape[0]
    wide = own.shape[1] // pieces
    copies = []
    for i in range(pieces):
        columns = slice(i * wide, (i + 1) * wide)
        added = dot(received[...], matrix[:, columns], ((1,), (0,)))
        out[i] = (own[:, columns] + added).astype(BF16)
        copies.append(pltpu.make_async_copy(out.at[i], far.at[:, columns], sems.at[i]))
        copies[-1].start()
    for copy in copies:
        copy.wait()


VMEM = 67043328
IN_VMEM = pl.BlockSpec(memory_space=pltpu.VMEM)
IN_HBM = pl.BlockSpec(memory_space=pltpu.HBM)


def call(kernel, name, far, near, outs, flops, scratch=(), left=24 << 20, out_spec=IN_VMEM):
    inputs = (*far, *near)
    moved = sum(a.size * a.dtype.itemsize for a in (*inputs, *outs))
    results = pl.pallas_call(
        kernel,
        name=name,
        out_shape=outs,
        in_specs=[IN_HBM] * len(far) + [IN_VMEM] * len(near),
        out_specs=[out_spec] * len(outs),
        scratch_shapes=scratch,
        compiler_params=pltpu.CompilerParams(vmem_limit_bytes=VMEM - left),
        cost_estimate=pl.CostEstimate(flops=flops, bytes_accessed=moved, transcendentals=0),
    )(*inputs)
    return results if len(outs) > 1 else results[0]


def body(
    probe_preactivation,
    retention_preactivation,
    source_entries,
    extra_log_retention,
    retention_slack,
    group_normalizer_gain,
    readout_mapping_matrix,
):
    tokens, channels = probe_preactivation.shape
    heads = channels // HEAD
    positions = lax.axis_size(SP)
    slabs = positions // heads
    rows = HEAD // slabs
    width = readout_mapping_matrix.shape[1]
    slack = retention_slack.reshape(1, channels)
    gain = group_normalizer_gain.reshape(1, HEAD)
    extra = extra_log_retention.T
    flops = 2 * tokens * channels * HEAD
    retention, source, extra, slack, probe = (
        lax.ppermute(a, "tp", STAY)
        for a in (
            retention_preactivation,
            source_entries,
            extra,
            slack,
            probe_preactivation,
        )
    )
    retention, source, partner_matrix = lax.optimization_barrier(
        (retention, source, readout_mapping_matrix)
    )
    partner_matrix = lax.ppermute(partner_matrix, "tp", SWAP)
    message = call(
        functools.partial(state_kernel, slabs),
        "state",
        (),
        (retention, source, extra, slack),
        [jax.ShapeDtypeStruct((positions, rows + 8, HEAD), BF16)],
        4 * flops,
    )
    arrived = lax.all_to_all(message, SP, split_axis=0, concat_axis=0, tiled=True)
    inside, reading = call(
        local_kernel,
        "local",
        (),
        (probe, retention, source, extra, slack),
        [
            jax.ShapeDtypeStruct((tokens, channels), F32),
            jax.ShapeDtypeStruct((tokens, channels), BF16),
        ],
        6 * flops,
    )
    arrived, inside, reading, matrix, partner_matrix = lax.optimization_barrier(
        (arrived, inside, reading, readout_mapping_matrix, partner_matrix)
    )
    matrix = lax.ppermute(matrix, "tp", STAY)
    partner_matrix = lax.ppermute(partner_matrix, "tp", STAY)
    scanned = call(
        functools.partial(scan_kernel, slabs),
        "scan",
        (),
        (arrived,),
        [jax.ShapeDtypeStruct((positions, rows, HEAD), BF16)],
        flops,
        [pltpu.VMEM((HEAD, positions), F32)],
    )
    entering = lax.all_to_all(scanned, SP, split_axis=0, concat_axis=0, tiled=True)
    entering = entering.reshape(heads, HEAD, HEAD)
    half = tokens // lax.axis_size("tp")

    projection = half * channels * width * 2
    mine, other = call(
        norm_kernel,
        "norm",
        (),
        (inside, reading, entering, gain),
        [jax.ShapeDtypeStruct((half, channels), BF16)] * 2,
        flops,
    )
    received = lax.ppermute(other, "tp", SWAP)
    pieces = 4
    own = call(
        own_kernel,
        "own",
        (),
        (mine, matrix),
        [jax.ShapeDtypeStruct((half, width), F32)],
        projection,
    )
    return call(
        final_kernel,
        "final",
        (),
        (own, received, partner_matrix),
        [jax.ShapeDtypeStruct((half, width), BF16)],
        projection,
        [pltpu.VMEM((pieces, half, width // pieces), BF16), pltpu.SemaphoreType.DMA((pieces,))],
        out_spec=IN_HBM,
    )


def solution(mesh):
    finer = Mesh(
        mesh.devices.reshape(mesh.shape["grp"], 8, 8, mesh.shape["tp"]),
        ("grp", "sp_0", "sp_1", "tp"),
    )
    in_specs = (
        P(GRP_SP, "tp"),
        P(GRP_SP, "tp"),
        P(GRP_SP, "tp"),
        P(GRP_SP, "tp"),
        P("tp"),
        P(),
        P("tp", None),
    )
    out_specs = P(GRP_SP_TP, None)
    return jax.shard_map(body, mesh=finer, in_specs=in_specs, out_specs=out_specs, check_vma=False)
```

```python
import functools

import jax
import jax.numpy as jnp
from jax import lax
from jax.experimental import pallas as pl
from jax.experimental.pallas import tpu as pltpu
from jax.sharding import Mesh
from jax.sharding import PartitionSpec as P

SPAN = 128
HEAD = 128
SP = ("sp_0", "sp_1")
GRP_SP = ("grp", "sp_0", "sp_1")
GRP_SP_TP = ("grp", "sp_0", "sp_1", "tp")
F32 = jnp.float32
BF16 = jnp.bfloat16


def dot(a, b, contract):
    return lax.dot_general(a, b, (contract, ((), ())), preferred_element_type=F32)


def two_parts(x):
    high = x.astype(BF16)
    return high, (x - high.astype(F32)).astype(BF16)


def summed_rows(selection, x):
    return sum(dot(selection, part, ((1,), (0,))) for part in two_parts(x))


def keyed_and_log_decay(retention, slack, extra):
    keyed = slack * jax.nn.sigmoid(-retention.astype(F32))
    return keyed, jnp.log1p(-keyed) + extra


def rows_and_columns(shape):
    return lax.broadcasted_iota(jnp.int32, shape, 0), lax.broadcasted_iota(jnp.int32, shape, 1)


def state_kernel(
    slabs, retention, source, far_extra, far_slack, message, r_in, v_in, extra, slack, sems, small
):
    tokens, channels = retention.shape
    wide = 2 * HEAD
    pairs = channels // wide
    first = [
        pltpu.make_async_copy(a, b, small.at[i])
        for i, (a, b) in enumerate(((far_extra, extra), (far_slack, slack)))
    ]
    for copy in first:
        copy.start()

    def copies(source_ref, target, row):
        return [
            pltpu.make_async_copy(
                source_ref.at[:, p * wide : (p + 1) * wide], target.at[p], sems.at[row, p]
            )
            for p in range(pairs)
        ]

    r_copies, v_copies = (copies(retention, r_in, 0), copies(source, v_in, 1))
    for p in range(pairs):
        r_copies[p].start()
        v_copies[p].start()
    r, c = rows_and_columns((tokens, tokens))
    later = (c > r).astype(BF16)
    rows = HEAD // slabs
    for copy in first:
        copy.wait()
    by_token = extra[...].T
    for p in range(pairs):
        r_copies[p].wait()
        added = jnp.concatenate(
            [
                jnp.broadcast_to(by_token[:, h : h + 1], (tokens, HEAD))
                for h in (2 * p, 2 * p + 1)
            ],
            axis=1,
        )
        keyed, log_decay = keyed_and_log_decay(
            r_in[p], slack[:, p * wide : (p + 1) * wide], added
        )
        ahead = summed_rows(later, log_decay)
        sent = (keyed * jnp.exp(ahead)).astype(BF16)
        total = ahead[:1] + log_decay[:1]
        parts = jnp.concatenate(two_parts(total) + (jnp.zeros((6, wide), BF16),), axis=0)
        v_copies[p].wait()
        for k in range(2):
            lanes = slice(k * HEAD, (k + 1) * HEAD)
            h = 2 * p + k
            state = dot(sent[:, lanes], v_in[p, :, lanes], ((0,), (0,)))
            message[h * slabs : (h + 1) * slabs, :rows, :] = state.astype(BF16).reshape(
                slabs, rows, HEAD
            )
            message[h * slabs : (h + 1) * slabs, rows:, :] = jnp.broadcast_to(
                parts[None, :, lanes], (slabs, 8, HEAD)
            )


def scan_kernel(slabs, message, entering, by_channel):
    positions, rows, _ = entering.shape
    slab = lax.rem(lax.axis_index(SP), slabs)
    parts = message[:, rows:, :].astype(F32)
    by_channel[...] = jnp.exp(parts[:, 0] + parts[:, 1]).T
    mine = by_channel[pl.ds(pl.multiple_of(slab * rows, rows), rows), :]
    state = jnp.zeros((rows, HEAD), F32)
    for i in range(positions):
        entering[i] = state.astype(BF16)
        if i + 1 < positions:
            state = mine[:, i : i + 1] * state + message[i, :rows, :].astype(F32)


def local_kernel(probe, retention, source, extra, slack, inside, reading):
    tokens, channels = retention.shape
    r, c = rows_and_columns((SPAN, SPAN))
    upto = c <= r
    upto_ones = upto.astype(BF16)
    by_token = extra[...].T
    for h in range(channels // HEAD):
        lanes = slice(h * HEAD, (h + 1) * HEAD)
        before, decayed = None, None
        for b in range(tokens // SPAN):
            span = slice(b * SPAN, (b + 1) * SPAN)
            keyed, log_decay = keyed_and_log_decay(
                retention[span, lanes], slack[:, lanes], by_token[span, h : h + 1]
            )
            values = source[span, lanes]
            query = jax.nn.silu(probe[span, lanes].astype(F32))
            running = summed_rows(upto_ones, log_decay)
            last = running[SPAN - 1 :]
            raised = query * jnp.exp(running)
            lifted = raised.astype(BF16)
            lowered = (keyed * jnp.exp(-running)).astype(BF16)
            scores = dot(lifted, lowered, ((1,), (1,)))
            weights = jnp.where(upto, scores, 0.0).astype(BF16)
            out = dot(weights, values, ((1,), (0,)))
            if before is not None:
                out = out + dot(lifted, before.astype(BF16), ((1,), (0,)))
                reading[span, lanes] = (query * jnp.exp(running + decayed)).astype(BF16)
            else:
                reading[span, lanes] = lifted
            inside[span, lanes] = out
            if (b + 1) * SPAN < tokens:
                sent = (keyed * jnp.exp(last - running)).astype(BF16)
                added = dot(sent, values, ((0,), (0,)))
                if before is None:
                    before, decayed = added, last
                else:
                    before = jnp.exp(last).reshape(HEAD, 1) * before + added
                    decayed = decayed + last


def output_kernel(away, inside, reading, entering, gain, matrix, out, normed):
    tokens = out.shape[0]
    mine = lax.axis_index("tp")
    half = 1 - mine if away else mine
    rows = pl.ds(pl.multiple_of(half * tokens, tokens), tokens)
    for h in range(entering.shape[0]):
        lanes = slice(h * HEAD, (h + 1) * HEAD)
        mixer = inside[rows, lanes] + dot(reading[rows, lanes], entering[h], ((1,), (0,)))
        scale = lax.rsqrt(jnp.mean(mixer * mixer, axis=-1, keepdims=True) + 1e-06)
        normed[:, lanes] = (mixer * scale * gain[...]).astype(BF16)
    out[...] = dot(normed[...], matrix[...], ((1,), (0,))).astype(out.dtype)


VMEM = 67043328
IN_VMEM = pl.BlockSpec(memory_space=pltpu.VMEM)
IN_HBM = pl.BlockSpec(memory_space=pltpu.HBM)


def call(kernel, name, far, near, outs, flops, scratch=(), left=24 << 20):
    inputs = (*far, *near)
    moved = sum(a.size * a.dtype.itemsize for a in (*inputs, *outs))
    results = pl.pallas_call(
        kernel,
        name=name,
        out_shape=outs,
        in_specs=[IN_HBM] * len(far) + [IN_VMEM] * len(near),
        out_specs=[IN_VMEM] * len(outs),
        scratch_shapes=scratch,
        compiler_params=pltpu.CompilerParams(vmem_limit_bytes=VMEM - left),
        cost_estimate=pl.CostEstimate(flops=flops, bytes_accessed=moved, transcendentals=0),
    )(*inputs)
    return results if len(outs) > 1 else results[0]


def body(
    probe_preactivation,
    retention_preactivation,
    source_entries,
    extra_log_retention,
    retention_slack,
    group_normalizer_gain,
    readout_mapping_matrix,
):
    tokens, channels = probe_preactivation.shape
    heads = channels // HEAD
    positions = lax.axis_size(SP)
    slabs = positions // heads
    rows = HEAD // slabs
    width = readout_mapping_matrix.shape[1]
    slack = retention_slack.reshape(1, channels)
    gain = group_normalizer_gain.reshape(1, HEAD)
    extra = extra_log_retention.T
    flops = 2 * tokens * channels * HEAD
    pairs = channels // (2 * HEAD)

    message = call(
        functools.partial(state_kernel, slabs),
        "state",
        (retention_preactivation, source_entries, extra, slack),
        (),
        [jax.ShapeDtypeStruct((positions, rows + 8, HEAD), BF16)],
        4 * flops,
        [pltpu.VMEM((pairs, tokens, 2 * HEAD), BF16)] * 2
        + [pltpu.VMEM(extra.shape, F32), pltpu.VMEM(slack.shape, F32)]
        + [pltpu.SemaphoreType.DMA((2, pairs)), pltpu.SemaphoreType.DMA((2,))],
        0,
    )
    arrived = lax.all_to_all(message, SP, split_axis=0, concat_axis=0, tiled=True)
    inside, reading = call(
        local_kernel,
        "local",
        (),
        (probe_preactivation, retention_preactivation, source_entries, extra, slack),
        [
            jax.ShapeDtypeStruct((tokens, channels), F32),
            jax.ShapeDtypeStruct((tokens, channels), BF16),
        ],
        6 * flops,
    )
    arrived, inside, reading = lax.optimization_barrier((arrived, inside, reading))
    scanned = call(
        functools.partial(scan_kernel, slabs),
        "scan",
        (),
        (arrived,),
        [jax.ShapeDtypeStruct((positions, rows, HEAD), BF16)],
        40 * flops,
        [pltpu.VMEM((HEAD, positions), F32)],
    )
    entering = lax.all_to_all(scanned, SP, split_axis=0, concat_axis=0, tiled=True)
    entering = entering.reshape(heads, HEAD, HEAD)
    half = tokens // lax.axis_size("tp")

    def projected(away, dtype):
        return call(
            functools.partial(output_kernel, away),
            "away" if away else "kept",
            (),
            (inside, reading, entering, gain, readout_mapping_matrix),
            [jax.ShapeDtypeStruct((half, width), dtype)],
            half * channels * width * 2,
            [pltpu.VMEM((half, channels), BF16)],
        )

    received = lax.ppermute(projected(True, BF16), "tp", [(0, 1), (1, 0)])
    return (projected(False, F32) + received.astype(F32)).astype(BF16)


def solution(mesh):
    finer = Mesh(
        mesh.devices.reshape(mesh.shape["grp"], 8, 8, mesh.shape["tp"]),
        ("grp", "sp_0", "sp_1", "tp"),
    )
    in_specs = (
        P(GRP_SP, "tp"),
        P(GRP_SP, "tp"),
        P(GRP_SP, "tp"),
        P(GRP_SP, "tp"),
        P("tp"),
        P(),
        P("tp", None),
    )
    out_specs = P(GRP_SP_TP, None)
    return jax.shard_map(body, mesh=finer, in_specs=in_specs, out_specs=out_specs, check_vma=False)
```

```python
import functools

import jax
import jax.numpy as jnp
from jax import lax
from jax.experimental import pallas as pl
from jax.experimental.pallas import tpu as pltpu
from jax.sharding import Mesh
from jax.sharding import PartitionSpec as P

SPAN = 128
HEAD = 128
SP = ("sp_0", "sp_1")
GRP_SP = ("grp", "sp_0", "sp_1")
GRP_SP_TP = ("grp", "sp_0", "sp_1", "tp")
F32 = jnp.float32
BF16 = jnp.bfloat16


def dot(a, b, contract):
    return lax.dot_general(a, b, (contract, ((), ())), preferred_element_type=F32)


def two_parts(x):
    high = x.astype(BF16)
    return high, (x - high.astype(F32)).astype(BF16)


def summed_rows(selection, x):
    return sum(dot(selection, part, ((1,), (0,))) for part in two_parts(x))


def keyed_and_log_decay(retention, slack, extra):
    keyed = slack * jax.nn.sigmoid(-retention.astype(F32))
    return keyed, jnp.log1p(-keyed) + extra


def rows_and_columns(shape):
    return lax.broadcasted_iota(jnp.int32, shape, 0), lax.broadcasted_iota(jnp.int32, shape, 1)


def copied(pairs, sems):
    copies = [pltpu.make_async_copy(a, b, sems.at[i]) for i, (a, b) in enumerate(pairs)]
    for copy in copies:
        copy.start()
    return copies


def state_kernel(slabs, far, message, near, sems):
    copies = copied(zip(far, near), sems)
    retention, source, extra, slack = near
    tokens, channels = retention.shape
    wide = 2 * HEAD
    rows = HEAD // slabs
    r, c = rows_and_columns((tokens, tokens))
    later = (c > r).astype(BF16)
    for copy in copies:
        copy.wait()
    by_token = extra[...].T
    for p in range(channels // wide):
        lanes = slice(p * wide, (p + 1) * wide)
        added = jnp.concatenate(
            [
                jnp.broadcast_to(by_token[:, h : h + 1], (tokens, HEAD))
                for h in (2 * p, 2 * p + 1)
            ],
            axis=1,
        )
        keyed, log_decay = keyed_and_log_decay(retention[:, lanes], slack[:, lanes], added)
        ahead = summed_rows(later, log_decay)
        sent = (keyed * jnp.exp(ahead)).astype(BF16)
        total = ahead[:1] + log_decay[:1]
        parts = jnp.concatenate(two_parts(total) + (jnp.zeros((6, wide), BF16),), axis=0)
        for k in range(2):
            part = slice(k * HEAD, (k + 1) * HEAD)
            h = 2 * p + k
            values = source[:, h * HEAD : (h + 1) * HEAD]
            state = dot(sent[:, part], values, ((0,), (0,)))
            message[h * slabs : (h + 1) * slabs, :rows, :] = state.astype(BF16).reshape(
                slabs, rows, HEAD
            )
            message[h * slabs : (h + 1) * slabs, rows:, :] = jnp.broadcast_to(
                parts[None, :, part], (slabs, 8, HEAD)
            )


def scan_kernel(slabs, message, entering, by_channel):
    positions, rows, _ = entering.shape
    slab = lax.rem(lax.axis_index(SP), slabs)
    parts = message[:, rows:, :].astype(F32)
    by_channel[...] = jnp.exp(parts[:, 0] + parts[:, 1]).T
    mine = by_channel[pl.ds(pl.multiple_of(slab * rows, rows), rows), :]
    state = jnp.zeros((rows, HEAD), F32)
    for i in range(positions):
        entering[i] = state.astype(BF16)
        if i + 1 < positions:
            state = mine[:, i : i + 1] * state + message[i, :rows, :].astype(F32)


def local_kernel(far, inside, reading, near, sems):
    copies = copied(zip(far, near), sems)
    retention, source, extra, slack, probe = near
    tokens, channels = retention.shape
    r, c = rows_and_columns((SPAN, SPAN))
    upto = c <= r
    upto_ones = upto.astype(BF16)
    for copy in copies:
        copy.wait()
    by_token = extra[...].T
    for h in range(channels // HEAD):
        lanes = slice(h * HEAD, (h + 1) * HEAD)
        before, decayed = None, None
        for b in range(tokens // SPAN):
            span = slice(b * SPAN, (b + 1) * SPAN)
            keyed, log_decay = keyed_and_log_decay(
                retention[span, lanes], slack[:, lanes], by_token[span, h : h + 1]
            )
            values = source[span, lanes]
            query = jax.nn.silu(probe[span, lanes].astype(F32))
            running = summed_rows(upto_ones, log_decay)
            last = running[SPAN - 1 :]
            raised = query * jnp.exp(running)
            lifted = raised.astype(BF16)
            lowered = (keyed * jnp.exp(-running)).astype(BF16)
            scores = dot(lifted, lowered, ((1,), (1,)))
            weights = jnp.where(upto, scores, 0.0).astype(BF16)
            out = dot(weights, values, ((1,), (0,)))
            if before is not None:
                out = out + dot(lifted, before.astype(BF16), ((1,), (0,)))
                reading[span, lanes] = (query * jnp.exp(running + decayed)).astype(BF16)
            else:
                reading[span, lanes] = lifted
            inside[span, lanes] = out.astype(BF16)
            if (b + 1) * SPAN < tokens:
                sent = (keyed * jnp.exp(last - running)).astype(BF16)
                added = dot(sent, values, ((0,), (0,)))
                if before is None:
                    before, decayed = added, last
                else:
                    before = jnp.exp(last).reshape(HEAD, 1) * before + added
                    decayed = decayed + last


def output_kernel(away, inside, reading, entering, gain, matrix, out, normed):
    tokens = out.shape[0]
    mine = lax.axis_index("tp")
    half = 1 - mine if away else mine
    rows = pl.ds(pl.multiple_of(half * tokens, tokens), tokens)
    for h in range(entering.shape[0]):
        lanes = slice(h * HEAD, (h + 1) * HEAD)
        mixer = inside[rows, lanes] + dot(reading[rows, lanes], entering[h], ((1,), (0,)))
        scale = lax.rsqrt(jnp.mean(mixer * mixer, axis=-1, keepdims=True) + 1e-06)
        normed[:, lanes] = (mixer * scale * gain[...]).astype(BF16)
    out[...] = dot(normed[...], matrix[...], ((1,), (0,))).astype(out.dtype)


VMEM = 67043328
IN_VMEM = pl.BlockSpec(memory_space=pltpu.VMEM)
IN_HBM = pl.BlockSpec(memory_space=pltpu.HBM)


def call(kernel, name, far, near, outs, flops, scratch=(), left=24 << 20):
    inputs = (*far, *near)
    moved = sum(a.size * a.dtype.itemsize for a in (*inputs, *outs))
    results = pl.pallas_call(
        kernel,
        name=name,
        out_shape=outs,
        in_specs=[IN_HBM] * len(far) + [IN_VMEM] * len(near),
        out_specs=[IN_VMEM] * len(outs),
        scratch_shapes=list(scratch),
        compiler_params=pltpu.CompilerParams(vmem_limit_bytes=VMEM - left),
        cost_estimate=pl.CostEstimate(flops=flops, bytes_accessed=moved, transcendentals=0),
    )(*inputs)
    return results if len(outs) > 1 else results[0]


def body(
    probe_preactivation,
    retention_preactivation,
    source_entries,
    extra_log_retention,
    retention_slack,
    group_normalizer_gain,
    readout_mapping_matrix,
):
    tokens, channels = probe_preactivation.shape
    heads = channels // HEAD
    positions = lax.axis_size(SP)
    slabs = positions // heads
    rows = HEAD // slabs
    width = readout_mapping_matrix.shape[1]
    slack = retention_slack.reshape(1, channels)
    gain = group_normalizer_gain.reshape(1, HEAD)
    extra = extra_log_retention.T
    flops = 2 * tokens * channels * HEAD
    inputs = (retention_preactivation, source_entries, extra, slack)

    def near(arrays):
        return (
            tuple(pltpu.VMEM(a.shape, a.dtype) for a in arrays),
            pltpu.SemaphoreType.DMA((len(arrays),)),
        )

    message = call(
        lambda *refs: state_kernel(slabs, refs[:4], *refs[4:]),
        "state",
        inputs,
        (),
        [jax.ShapeDtypeStruct((positions, rows + 8, HEAD), BF16)],
        4 * flops,
        near(inputs),
        0,
    )
    arrived = lax.all_to_all(message, SP, split_axis=0, concat_axis=0, tiled=True)
    inputs = (*inputs, probe_preactivation)
    inside, reading = call(
        lambda *refs: local_kernel(refs[:5], *refs[5:]),
        "local",
        inputs,
        (),
        [jax.ShapeDtypeStruct((tokens, channels), BF16)] * 2,
        6 * flops,
        near(inputs),
        21 << 19,
    )
    arrived, inside, reading = lax.optimization_barrier((arrived, inside, reading))
    scanned = call(
        functools.partial(scan_kernel, slabs),
        "scan",
        (),
        (arrived,),
        [jax.ShapeDtypeStruct((positions, rows, HEAD), BF16)],
        40 * flops,
        [pltpu.VMEM((HEAD, positions), F32)],
    )
    entering = lax.all_to_all(scanned, SP, split_axis=0, concat_axis=0, tiled=True)
    entering = entering.reshape(heads, HEAD, HEAD)
    half = tokens // lax.axis_size("tp")

    def projected(away, dtype):
        return call(
            functools.partial(output_kernel, away),
            "away" if away else "kept",
            (),
            (inside, reading, entering, gain, readout_mapping_matrix),
            [jax.ShapeDtypeStruct((half, width), dtype)],
            half * channels * width * 2,
            [pltpu.VMEM((half, channels), BF16)],
        )

    received = lax.ppermute(projected(True, BF16), "tp", [(0, 1), (1, 0)])
    return (projected(False, F32) + received.astype(F32)).astype(BF16)


def solution(mesh):
    finer = Mesh(
        mesh.devices.reshape(mesh.shape["grp"], 8, 8, mesh.shape["tp"]),
        ("grp", "sp_0", "sp_1", "tp"),
    )
    in_specs = (
        P(GRP_SP, "tp"),
        P(GRP_SP, "tp"),
        P(GRP_SP, "tp"),
        P(GRP_SP, "tp"),
        P("tp"),
        P(),
        P("tp", None),
    )
    out_specs = P(GRP_SP_TP, None)
    return jax.shard_map(body, mesh=finer, in_specs=in_specs, out_specs=out_specs, check_vma=False)
```

```python
import functools

import jax
import jax.numpy as jnp
from jax import lax
from jax.experimental import pallas as pl
from jax.experimental.pallas import tpu as pltpu
from jax.sharding import Mesh
from jax.sharding import PartitionSpec as P

SPAN = 128
HEAD = 128
SP = ("sp_0", "sp_1")
GRP_SP = ("grp", "sp_0", "sp_1")
GRP_SP_TP = ("grp", "sp_0", "sp_1", "tp")
F32 = jnp.float32
BF16 = jnp.bfloat16


def dot(a, b, contract):
    return lax.dot_general(a, b, (contract, ((), ())), preferred_element_type=F32)


def two_parts(x):
    high = x.astype(BF16)
    return high, (x - high.astype(F32)).astype(BF16)


def summed_rows(selection, x):
    return sum(dot(selection, part, ((1,), (0,))) for part in two_parts(x))


def keyed_and_log_decay(retention, slack, extra):
    keyed = slack * jax.nn.sigmoid(-retention.astype(F32))
    return keyed, jnp.log(1.0 - keyed) + extra


def rows_and_columns(shape):
    return lax.broadcasted_iota(jnp.int32, shape, 0), lax.broadcasted_iota(jnp.int32, shape, 1)


def for_pair(by_token, p):
    return jnp.concatenate(
        [
            jnp.broadcast_to(by_token[:, h : h + 1], (by_token.shape[0], HEAD))
            for h in (2 * p, 2 * p + 1)
        ],
        axis=1,
    )


def copied(pairs, sems):
    copies = [pltpu.make_async_copy(a, b, sems.at[i]) for i, (a, b) in enumerate(pairs)]
    for copy in copies:
        copy.start()
    return copies


def staggered(make, count):
    chains = [make(i) for i in range(count)]
    live = []
    while chains or live:
        if chains:
            live.append(chains.pop(0))
        live = [chain for chain in live if next(chain, live) is None]


def state_kernel(slabs, far, message, near, sems):
    copies = copied(zip(far, near), sems)
    retention, source, extra, slack = near
    tokens, channels = retention.shape
    wide = 2 * HEAD
    rows = HEAD // slabs
    r, c = rows_and_columns((tokens, tokens))
    later = (c > r).astype(BF16)
    for copy in copies:
        copy.wait()
    by_token = extra[...].T

    def chain(p):
        lanes = slice(p * wide, (p + 1) * wide)
        keyed, log_decay = keyed_and_log_decay(
            retention[:, lanes], slack[:, lanes], for_pair(by_token, p)
        )
        yield
        ahead = summed_rows(later, log_decay)
        yield
        sent = (keyed * jnp.exp(ahead)).astype(BF16)
        total = ahead[:1] + log_decay[:1]
        parts = jnp.concatenate(two_parts(total) + (jnp.zeros((6, wide), BF16),), axis=0)
        yield
        for k in range(2):
            part = slice(k * HEAD, (k + 1) * HEAD)
            h = 2 * p + k
            values = source[:, h * HEAD : (h + 1) * HEAD]
            state = dot(sent[:, part], values, ((0,), (0,)))
            message[h * slabs : (h + 1) * slabs, :rows, :] = state.astype(BF16).reshape(
                slabs, rows, HEAD
            )
            message[h * slabs : (h + 1) * slabs, rows:, :] = jnp.broadcast_to(
                parts[None, :, part], (slabs, 8, HEAD)
            )

    staggered(chain, channels // wide)


def scan_kernel(slabs, message, entering, by_channel):
    positions, rows, _ = entering.shape
    slab = lax.rem(lax.axis_index(SP), slabs)
    parts = message[:, rows:, :].astype(F32)
    by_channel[...] = jnp.exp(parts[:, 0] + parts[:, 1]).T
    mine = by_channel[pl.ds(pl.multiple_of(slab * rows, rows), rows), :]
    state = jnp.zeros((rows, HEAD), F32)
    for i in range(positions):
        entering[i] = state.astype(BF16)
        if i + 1 < positions:
            state = mine[:, i : i + 1] * state + message[i, :rows, :].astype(F32)


def local_kernel(far, inside, reading, near, sems):
    copies = copied(zip(far, near), sems)
    retention, source, extra, slack, probe = near
    tokens, channels = retention.shape
    wide = 2 * HEAD
    r, c = rows_and_columns((tokens, tokens))
    within = ((c <= r) & (r // SPAN == c // SPAN)).astype(BF16)
    r, c = rows_and_columns((SPAN, SPAN))
    upto = c <= r
    for copy in copies:
        copy.wait()
    by_token = extra[...].T

    def chain(p):
        lanes = slice(p * wide, (p + 1) * wide)
        keyed, log_decay = keyed_and_log_decay(
            retention[:, lanes], slack[:, lanes], for_pair(by_token, p)
        )
        yield
        running = summed_rows(within, log_decay)
        yield
        raised = jax.nn.silu(probe[:, lanes].astype(F32)) * jnp.exp(running)
        lifted = raised.astype(BF16)
        lowered = (keyed * jnp.exp(-running)).astype(BF16)
        yield
        decayed, before = None, [None, None]
        for b in range(tokens // SPAN):
            span = slice(b * SPAN, (b + 1) * SPAN)
            last = running[(b + 1) * SPAN - 1 : (b + 1) * SPAN]
            if b == 0:
                reading[span, lanes] = lifted[span]
            else:
                reading[span, lanes] = (raised[span] * jnp.exp(decayed)).astype(BF16)
            more = (b + 1) * SPAN < tokens
            if more:
                sent = (keyed[span] * jnp.exp(last - running[span])).astype(BF16)
                decayed = last if b == 0 else decayed + last
            weights = []
            for k in range(2):
                part = slice(k * HEAD, (k + 1) * HEAD)
                scores = dot(lifted[span, part], lowered[span, part], ((1,), (1,)))
                weights.append(jnp.where(upto, scores, 0.0).astype(BF16))
            yield
            for k in range(2):
                part = slice(k * HEAD, (k + 1) * HEAD)
                columns = slice(p * wide + k * HEAD, p * wide + (k + 1) * HEAD)
                values = source[span, columns]
                left, right = weights[k], values
                if b > 0:
                    left = jnp.concatenate([left, lifted[span, part]], axis=1)
                    right = jnp.concatenate([right, before[k].astype(BF16)], axis=0)
                inside[span, columns] = dot(left, right, ((1,), (0,))).astype(BF16)
                if more:
                    added = dot(sent[:, part], values, ((0,), (0,)))
                    if b > 0:
                        added = jnp.exp(last[:, part]).reshape(HEAD, 1) * before[k] + added
                    before[k] = added
            yield

    staggered(chain, channels // wide)


def output_kernel(away, inside, reading, entering, gain, matrix, out, normed):
    tokens = out.shape[0]
    mine = lax.axis_index("tp")
    half = 1 - mine if away else mine
    rows = pl.ds(pl.multiple_of(half * tokens, tokens), tokens)
    for h in range(entering.shape[0]):
        lanes = slice(h * HEAD, (h + 1) * HEAD)
        mixer = inside[rows, lanes] + dot(reading[rows, lanes], entering[h], ((1,), (0,)))
        scale = lax.rsqrt(jnp.mean(mixer * mixer, axis=-1, keepdims=True) + 1e-06)
        normed[:, lanes] = (mixer * scale * gain[...]).astype(BF16)
    out[...] = dot(normed[...], matrix[...], ((1,), (0,))).astype(out.dtype)


VMEM = 67043328
IN_VMEM = pl.BlockSpec(memory_space=pltpu.VMEM)
IN_HBM = pl.BlockSpec(memory_space=pltpu.HBM)


def call(kernel, name, far, near, outs, flops, scratch=(), left=24 << 20):
    inputs = (*far, *near)
    moved = sum(a.size * a.dtype.itemsize for a in (*inputs, *outs))
    results = pl.pallas_call(
        kernel,
        name=name,
        out_shape=outs,
        in_specs=[IN_HBM] * len(far) + [IN_VMEM] * len(near),
        out_specs=[IN_VMEM] * len(outs),
        scratch_shapes=list(scratch),
        compiler_params=pltpu.CompilerParams(vmem_limit_bytes=VMEM - left),
        cost_estimate=pl.CostEstimate(flops=flops, bytes_accessed=moved, transcendentals=0),
    )(*inputs)
    return results if len(outs) > 1 else results[0]


def body(
    probe_preactivation,
    retention_preactivation,
    source_entries,
    extra_log_retention,
    retention_slack,
    group_normalizer_gain,
    readout_mapping_matrix,
):
    tokens, channels = probe_preactivation.shape
    heads = channels // HEAD
    positions = lax.axis_size(SP)
    slabs = positions // heads
    rows = HEAD // slabs
    width = readout_mapping_matrix.shape[1]
    slack = retention_slack.reshape(1, channels)
    gain = group_normalizer_gain.reshape(1, HEAD)
    extra = extra_log_retention.T
    flops = 2 * tokens * channels * HEAD
    inputs = (retention_preactivation, source_entries, extra, slack)

    def near(arrays):
        return (
            tuple(pltpu.VMEM(a.shape, a.dtype) for a in arrays),
            pltpu.SemaphoreType.DMA((len(arrays),)),
        )

    message = call(
        lambda *refs: state_kernel(slabs, refs[:4], *refs[4:]),
        "state",
        inputs,
        (),
        [jax.ShapeDtypeStruct((positions, rows + 8, HEAD), BF16)],
        4 * flops,
        near(inputs),
        0,
    )
    arrived = lax.all_to_all(message, SP, split_axis=0, concat_axis=0, tiled=True)
    inputs = (*inputs, probe_preactivation)
    inside, reading = call(
        lambda *refs: local_kernel(refs[:5], *refs[5:]),
        "local",
        inputs,
        (),
        [jax.ShapeDtypeStruct((tokens, channels), BF16)] * 2,
        6 * flops,
        near(inputs),
        21 << 19,
    )
    arrived, inside, reading = lax.optimization_barrier((arrived, inside, reading))
    scanned = call(
        functools.partial(scan_kernel, slabs),
        "scan",
        (),
        (arrived,),
        [jax.ShapeDtypeStruct((positions, rows, HEAD), BF16)],
        40 * flops,
        [pltpu.VMEM((HEAD, positions), F32)],
    )
    entering = lax.all_to_all(scanned, SP, split_axis=0, concat_axis=0, tiled=True)
    entering = entering.reshape(heads, HEAD, HEAD)
    half = tokens // lax.axis_size("tp")

    def projected(away, dtype):
        return call(
            functools.partial(output_kernel, away),
            "away" if away else "kept",
            (),
            (inside, reading, entering, gain, readout_mapping_matrix),
            [jax.ShapeDtypeStruct((half, width), dtype)],
            half * channels * width * 2,
            [pltpu.VMEM((half, channels), BF16)],
        )

    received = lax.ppermute(projected(True, BF16), "tp", [(0, 1), (1, 0)])
    return (projected(False, F32) + received.astype(F32)).astype(BF16)


def solution(mesh):
    finer = Mesh(
        mesh.devices.reshape(mesh.shape["grp"], 8, 8, mesh.shape["tp"]),
        ("grp", "sp_0", "sp_1", "tp"),
    )
    in_specs = (
        P(GRP_SP, "tp"),
        P(GRP_SP, "tp"),
        P(GRP_SP, "tp"),
        P(GRP_SP, "tp"),
        P("tp"),
        P(),
        P("tp", None),
    )
    out_specs = P(GRP_SP_TP, None)
    return jax.shard_map(body, mesh=finer, in_specs=in_specs, out_specs=out_specs, check_vma=False)
```

```python
import functools

import jax
import jax.numpy as jnp
from jax import lax
from jax.experimental import pallas as pl
from jax.experimental.pallas import tpu as pltpu
from jax.sharding import Mesh
from jax.sharding import PartitionSpec as P

SPAN = 128
HEAD = 128
SP = ("sp_0", "sp_1")
GRP_SP = ("grp", "sp_0", "sp_1")
GRP_SP_TP = ("grp", "sp_0", "sp_1", "tp")
F32 = jnp.float32
BF16 = jnp.bfloat16


def dot(a, b, contract):
    return lax.dot_general(a, b, (contract, ((), ())), preferred_element_type=F32)


def two_parts(x):
    high = x.astype(BF16)
    return high, (x - high.astype(F32)).astype(BF16)


def summed_rows(selection, x):
    return sum(dot(selection, part, ((1,), (0,))) for part in two_parts(x))


def keyed_and_log_decay(retention, slack, extra):
    keyed = slack * jax.nn.sigmoid(-retention.astype(F32))
    return keyed, jnp.log(1.0 - keyed) + extra


def rows_and_columns(shape):
    return lax.broadcasted_iota(jnp.int32, shape, 0), lax.broadcasted_iota(jnp.int32, shape, 1)


def for_pair(by_token, p):
    return jnp.concatenate(
        [
            jnp.broadcast_to(by_token[:, h : h + 1], (by_token.shape[0], HEAD))
            for h in (2 * p, 2 * p + 1)
        ],
        axis=1,
    )


def copied(pairs, sems):
    copies = [pltpu.make_async_copy(a, b, sems.at[i]) for i, (a, b) in enumerate(pairs)]
    for copy in copies:
        copy.start()
    return copies


def staggered(make, count):
    chains = [make(i) for i in range(count)]
    live = []
    while chains or live:
        if chains:
            live.append(chains.pop(0))
        live = [chain for chain in live if next(chain, live) is None]


def state_kernel(slabs, far, message, near, sems):
    copies = copied(zip(far, near), sems)
    retention, extra, slack, source = near
    tokens, channels = retention.shape
    wide = 2 * HEAD
    rows = HEAD // slabs
    r, c = rows_and_columns((tokens, tokens))
    later = (c > r).astype(BF16)
    for copy in copies[:-1]:
        copy.wait()
    by_token = extra[...].T

    def chain(p):
        lanes = slice(p * wide, (p + 1) * wide)
        keyed, log_decay = keyed_and_log_decay(
            retention[:, lanes], slack[:, lanes], for_pair(by_token, p)
        )
        yield
        ahead = summed_rows(later, log_decay)
        yield
        sent = (keyed * jnp.exp(ahead)).astype(BF16)
        total = ahead[:1] + log_decay[:1]
        parts = jnp.concatenate(two_parts(total) + (jnp.zeros((6, wide), BF16),), axis=0)
        yield
        if p == 0:
            copies[-1].wait()
        for k in range(2):
            part = slice(k * HEAD, (k + 1) * HEAD)
            h = 2 * p + k
            values = source[:, h * HEAD : (h + 1) * HEAD]
            state = dot(sent[:, part], values, ((0,), (0,)))
            message[h * slabs : (h + 1) * slabs, :rows, :] = state.astype(BF16).reshape(
                slabs, rows, HEAD
            )
            message[h * slabs : (h + 1) * slabs, rows:, :] = jnp.broadcast_to(
                parts[None, :, part], (slabs, 8, HEAD)
            )

    staggered(chain, channels // wide)


def scan_kernel(slabs, message, entering, by_channel):
    positions, rows, _ = entering.shape
    slab = lax.rem(lax.axis_index(SP), slabs)
    parts = message[:, rows:, :].astype(F32)
    by_channel[...] = jnp.exp(parts[:, 0] + parts[:, 1]).T
    mine = by_channel[pl.ds(pl.multiple_of(slab * rows, rows), rows), :]
    state = jnp.zeros((rows, HEAD), F32)
    for i in range(positions):
        entering[i] = state.astype(BF16)
        if i + 1 < positions:
            state = mine[:, i : i + 1] * state + message[i, :rows, :].astype(F32)


def local_kernel(far, inside, reading, near, sems):
    copies = copied(zip(far, near), sems)
    retention, extra, slack, source, probe = near
    tokens, channels = retention.shape
    wide = 2 * HEAD
    r, c = rows_and_columns((tokens, tokens))
    within = ((c <= r) & (r // SPAN == c // SPAN)).astype(BF16)
    r, c = rows_and_columns((SPAN, SPAN))
    upto = c <= r
    for copy in copies:
        copy.wait()
    by_token = extra[...].T

    def chain(p):
        lanes = slice(p * wide, (p + 1) * wide)
        keyed, log_decay = keyed_and_log_decay(
            retention[:, lanes], slack[:, lanes], for_pair(by_token, p)
        )
        yield
        running = summed_rows(within, log_decay)
        yield
        raised = jax.nn.silu(probe[:, lanes].astype(F32)) * jnp.exp(running)
        lifted = raised.astype(BF16)
        lowered = (keyed * jnp.exp(-running)).astype(BF16)
        yield
        decayed, before = None, [None, None]
        for b in range(tokens // SPAN):
            span = slice(b * SPAN, (b + 1) * SPAN)
            last = running[(b + 1) * SPAN - 1 : (b + 1) * SPAN]
            if b == 0:
                reading[span, lanes] = lifted[span]
            else:
                reading[span, lanes] = (raised[span] * jnp.exp(decayed)).astype(BF16)
            more = (b + 1) * SPAN < tokens
            if more:
                sent = (keyed[span] * jnp.exp(last - running[span])).astype(BF16)
                decayed = last if b == 0 else decayed + last
            weights = []
            for k in range(2):
                part = slice(k * HEAD, (k + 1) * HEAD)
                scores = dot(lifted[span, part], lowered[span, part], ((1,), (1,)))
                weights.append(jnp.where(upto, scores, 0.0).astype(BF16))
            yield
            for k in range(2):
                part = slice(k * HEAD, (k + 1) * HEAD)
                columns = slice(p * wide + k * HEAD, p * wide + (k + 1) * HEAD)
                values = source[span, columns]
                left, right = weights[k], values
                if b > 0:
                    left = jnp.concatenate([left, lifted[span, part]], axis=1)
                    right = jnp.concatenate([right, before[k].astype(BF16)], axis=0)
                inside[span, columns] = dot(left, right, ((1,), (0,))).astype(BF16)
                if more:
                    added = dot(sent[:, part], values, ((0,), (0,)))
                    if b > 0:
                        added = jnp.exp(last[:, part]).reshape(HEAD, 1) * before[k] + added
                    before[k] = added
            yield

    staggered(chain, channels // wide)


def output_kernel(away, inside, reading, entering, gain, matrix, out, normed):
    tokens = out.shape[0]
    mine = lax.axis_index("tp")
    half = 1 - mine if away else mine
    rows = pl.ds(pl.multiple_of(half * tokens, tokens), tokens)
    for h in range(entering.shape[0]):
        lanes = slice(h * HEAD, (h + 1) * HEAD)
        mixer = inside[rows, lanes] + dot(reading[rows, lanes], entering[h], ((1,), (0,)))
        scale = lax.rsqrt(jnp.mean(mixer * mixer, axis=-1, keepdims=True) + 1e-06)
        normed[:, lanes] = (mixer * scale * gain[...]).astype(BF16)
    out[...] = dot(normed[...], matrix[...], ((1,), (0,))).astype(out.dtype)


def final_kernel(kept, received, far, out, sems):
    pieces, rows, _ = out.shape
    copies = []
    for i in range(pieces):
        span = slice(i * rows, (i + 1) * rows)
        out[i] = (kept[span] + received[span].astype(F32)).astype(BF16)
        copies.append(pltpu.make_async_copy(out.at[i], far.at[span], sems.at[i]))
        copies[-1].start()
    for copy in copies:
        copy.wait()


VMEM = 67043328
IN_VMEM = pl.BlockSpec(memory_space=pltpu.VMEM)
IN_HBM = pl.BlockSpec(memory_space=pltpu.HBM)


def call(kernel, name, far, near, outs, flops, scratch=(), left=24 << 20, out_spec=IN_VMEM):
    inputs = (*far, *near)
    moved = sum(a.size * a.dtype.itemsize for a in (*inputs, *outs))
    results = pl.pallas_call(
        kernel,
        name=name,
        out_shape=outs,
        in_specs=[IN_HBM] * len(far) + [IN_VMEM] * len(near),
        out_specs=[out_spec] * len(outs),
        scratch_shapes=list(scratch),
        compiler_params=pltpu.CompilerParams(vmem_limit_bytes=VMEM - left),
        cost_estimate=pl.CostEstimate(flops=flops, bytes_accessed=moved, transcendentals=0),
    )(*inputs)
    return results if len(outs) > 1 else results[0]


def body(
    probe_preactivation,
    retention_preactivation,
    source_entries,
    extra_log_retention,
    retention_slack,
    group_normalizer_gain,
    readout_mapping_matrix,
):
    tokens, channels = probe_preactivation.shape
    heads = channels // HEAD
    positions = lax.axis_size(SP)
    slabs = positions // heads
    rows = HEAD // slabs
    width = readout_mapping_matrix.shape[1]
    slack = retention_slack.reshape(1, channels)
    gain = group_normalizer_gain.reshape(1, HEAD)
    extra = extra_log_retention.T
    flops = 2 * tokens * channels * HEAD
    inputs = (retention_preactivation, extra, slack, source_entries)

    def near(arrays):
        return (
            tuple(pltpu.VMEM(a.shape, a.dtype) for a in arrays),
            pltpu.SemaphoreType.DMA((len(arrays),)),
        )

    message = call(
        lambda *refs: state_kernel(slabs, refs[:4], *refs[4:]),
        "state",
        inputs,
        (),
        [jax.ShapeDtypeStruct((positions, rows + 8, HEAD), BF16)],
        4 * flops,
        near(inputs),
        0,
    )
    arrived = lax.all_to_all(message, SP, split_axis=0, concat_axis=0, tiled=True)
    inputs = (*inputs, probe_preactivation)
    inside, reading = call(
        lambda *refs: local_kernel(refs[:5], *refs[5:]),
        "local",
        inputs,
        (),
        [jax.ShapeDtypeStruct((tokens, channels), BF16)] * 2,
        6 * flops,
        near(inputs),
        10300000,
    )
    arrived, inside, reading = lax.optimization_barrier((arrived, inside, reading))
    scanned = call(
        functools.partial(scan_kernel, slabs),
        "scan",
        (),
        (arrived,),
        [jax.ShapeDtypeStruct((positions, rows, HEAD), BF16)],
        40 * flops,
        [pltpu.VMEM((HEAD, positions), F32)],
    )
    entering = lax.all_to_all(scanned, SP, split_axis=0, concat_axis=0, tiled=True)
    entering = entering.reshape(heads, HEAD, HEAD)
    half = tokens // lax.axis_size("tp")

    def projected(away, dtype):
        return call(
            functools.partial(output_kernel, away),
            "away" if away else "kept",
            (),
            (inside, reading, entering, gain, readout_mapping_matrix),
            [jax.ShapeDtypeStruct((half, width), dtype)],
            half * channels * width * 2,
            [pltpu.VMEM((half, channels), BF16)],
        )

    received = lax.ppermute(projected(True, BF16), "tp", [(0, 1), (1, 0)])
    pieces = 4
    return call(
        final_kernel,
        "final",
        (),
        (projected(False, F32), received),
        [jax.ShapeDtypeStruct((half, width), BF16)],
        half * width,
        [pltpu.VMEM((pieces, half // pieces, width), BF16), pltpu.SemaphoreType.DMA((pieces,))],
        out_spec=IN_HBM,
    )


def solution(mesh):
    finer = Mesh(
        mesh.devices.reshape(mesh.shape["grp"], 8, 8, mesh.shape["tp"]),
        ("grp", "sp_0", "sp_1", "tp"),
    )
    in_specs = (
        P(GRP_SP, "tp"),
        P(GRP_SP, "tp"),
        P(GRP_SP, "tp"),
        P(GRP_SP, "tp"),
        P("tp"),
        P(),
        P("tp", None),
    )
    out_specs = P(GRP_SP_TP, None)
    return jax.shard_map(body, mesh=finer, in_specs=in_specs, out_specs=out_specs, check_vma=False)
```

```python
import functools

import jax
import jax.numpy as jnp
from jax import lax
from jax.experimental import pallas as pl
from jax.experimental.pallas import tpu as pltpu
from jax.sharding import Mesh
from jax.sharding import PartitionSpec as P

SPAN = 128
HEAD = 128
SP = ("sp_0", "sp_1")
GRP_SP = ("grp", "sp_0", "sp_1")
GRP_SP_TP = ("grp", "sp_0", "sp_1", "tp")
F32 = jnp.float32
BF16 = jnp.bfloat16


def dot(a, b, contract):
    return lax.dot_general(a, b, (contract, ((), ())), preferred_element_type=F32)


def two_parts(x):
    high = x.astype(BF16)
    return high, (x - high.astype(F32)).astype(BF16)


def summed_rows(selection, x):
    return sum(dot(selection, part, ((1,), (0,))) for part in two_parts(x))


def keyed_and_log_decay(retention, slack, extra):
    keyed = slack * jax.nn.sigmoid(-retention.astype(F32))
    return keyed, jnp.log(1.0 - keyed) + extra


def rows_and_columns(shape):
    return lax.broadcasted_iota(jnp.int32, shape, 0), lax.broadcasted_iota(jnp.int32, shape, 1)


def for_pair(by_token, p):
    return jnp.concatenate(
        [
            jnp.broadcast_to(by_token[:, h : h + 1], (by_token.shape[0], HEAD))
            for h in (2 * p, 2 * p + 1)
        ],
        axis=1,
    )


def copied(pairs, sems):
    copies = [pltpu.make_async_copy(a, b, sems.at[i]) for i, (a, b) in enumerate(pairs)]
    for copy in copies:
        copy.start()
    return copies


def staggered(make, count):
    chains = [make(i) for i in range(count)]
    live = []
    while chains or live:
        if chains:
            live.append(chains.pop(0))
        live = [chain for chain in live if next(chain, live) is None]


def state_kernel(slabs, far, message, near, sems):
    copies = copied(zip(far, near), sems)
    retention, extra, slack, source = near
    tokens, channels = retention.shape
    wide = 2 * HEAD
    rows = HEAD // slabs
    r, c = rows_and_columns((tokens, tokens))
    later = (c > r).astype(BF16)
    for copy in copies[:-1]:
        copy.wait()
    by_token = extra[...].T

    def chain(p):
        lanes = slice(p * wide, (p + 1) * wide)
        keyed, log_decay = keyed_and_log_decay(
            retention[:, lanes], slack[:, lanes], for_pair(by_token, p)
        )
        yield
        ahead = summed_rows(later, log_decay)
        yield
        sent = (keyed * jnp.exp(ahead)).astype(BF16)
        total = ahead[:1] + log_decay[:1]
        parts = jnp.concatenate(two_parts(total), axis=0)
        yield
        if p == 0:
            copies[-1].wait()
        for k in range(2):
            part = slice(k * HEAD, (k + 1) * HEAD)
            h = 2 * p + k
            values = source[:, h * HEAD : (h + 1) * HEAD]
            state = dot(sent[:, part], values, ((0,), (0,)))
            message[h * slabs : (h + 1) * slabs, : rows // 2] = state.astype(BF16).reshape(
                slabs, rows // 2, 2, HEAD
            )
            message[h * slabs : (h + 1) * slabs, rows // 2] = jnp.broadcast_to(
                parts[None, :, part], (slabs, 2, HEAD)
            )

    staggered(chain, channels // wide)


def scan_kernel(slabs, message, entering, by_channel):
    positions, rows, _ = entering.shape
    slab = lax.rem(lax.axis_index(SP), slabs)
    parts = message[:, rows // 2].astype(F32)
    by_channel[...] = jnp.exp(parts[:, 0] + parts[:, 1]).T
    mine = by_channel[pl.ds(pl.multiple_of(slab * rows, rows), rows), :]
    state = jnp.zeros((rows, HEAD), F32)
    for i in range(positions):
        entering[i] = state.astype(BF16)
        if i + 1 < positions:
            state = mine[:, i : i + 1] * state + message[i, : rows // 2].astype(F32).reshape(rows, HEAD)


def local_kernel(far, inside, reading, near, sems):
    copies = copied(zip(far, near), sems)
    retention, extra, slack, source, probe = near
    tokens, channels = retention.shape
    wide = 2 * HEAD
    r, c = rows_and_columns((tokens, tokens))
    within = ((c <= r) & (r // SPAN == c // SPAN)).astype(BF16)
    r, c = rows_and_columns((SPAN, SPAN))
    upto = c <= r
    for copy in copies:
        copy.wait()
    by_token = extra[...].T

    def chain(p):
        lanes = slice(p * wide, (p + 1) * wide)
        keyed, log_decay = keyed_and_log_decay(
            retention[:, lanes], slack[:, lanes], for_pair(by_token, p)
        )
        yield
        running = summed_rows(within, log_decay)
        yield
        raised = jax.nn.silu(probe[:, lanes].astype(F32)) * jnp.exp(running)
        lifted = raised.astype(BF16)
        lowered = (keyed * jnp.exp(-running)).astype(BF16)
        yield
        decayed, before = None, [None, None]
        for b in range(tokens // SPAN):
            span = slice(b * SPAN, (b + 1) * SPAN)
            last = running[(b + 1) * SPAN - 1 : (b + 1) * SPAN]
            if b == 0:
                reading[span, lanes] = lifted[span]
            else:
                reading[span, lanes] = (raised[span] * jnp.exp(decayed)).astype(BF16)
            more = (b + 1) * SPAN < tokens
            if more:
                sent = (keyed[span] * jnp.exp(last - running[span])).astype(BF16)
                decayed = last if b == 0 else decayed + last
            weights = []
            for k in range(2):
                part = slice(k * HEAD, (k + 1) * HEAD)
                scores = dot(lifted[span, part], lowered[span, part], ((1,), (1,)))
                weights.append(jnp.where(upto, scores, 0.0).astype(BF16))
            yield
            for k in range(2):
                part = slice(k * HEAD, (k + 1) * HEAD)
                columns = slice(p * wide + k * HEAD, p * wide + (k + 1) * HEAD)
                values = source[span, columns]
                left, right = weights[k], values
                if b > 0:
                    left = jnp.concatenate([left, lifted[span, part]], axis=1)
                    right = jnp.concatenate([right, before[k].astype(BF16)], axis=0)
                inside[span, columns] = dot(left, right, ((1,), (0,))).astype(BF16)
                if more:
                    added = dot(sent[:, part], values, ((0,), (0,)))
                    if b > 0:
                        added = jnp.exp(last[:, part]).reshape(HEAD, 1) * before[k] + added
                    before[k] = added
            yield

    staggered(chain, channels // wide)


def output_kernel(away, inside, reading, entering, gain, matrix, out, normed):
    tokens = out.shape[0]
    mine = lax.axis_index("tp")
    half = 1 - mine if away else mine
    rows = pl.ds(pl.multiple_of(half * tokens, tokens), tokens)
    for h in range(entering.shape[0]):
        lanes = slice(h * HEAD, (h + 1) * HEAD)
        mixer = inside[rows, lanes] + dot(reading[rows, lanes], entering[h], ((1,), (0,)))
        scale = lax.rsqrt(jnp.mean(mixer * mixer, axis=-1, keepdims=True) + 1e-06)
        normed[:, lanes] = (mixer * scale * gain[...]).astype(BF16)
    out[...] = dot(normed[...], matrix[...], ((1,), (0,))).astype(out.dtype)


def final_kernel(kept, received, far, out, sems):
    pieces, rows, _ = out.shape
    copies = []
    for i in range(pieces):
        span = slice(i * rows, (i + 1) * rows)
        out[i] = (kept[span] + received[span].astype(F32)).astype(BF16)
        copies.append(pltpu.make_async_copy(out.at[i], far.at[span], sems.at[i]))
        copies[-1].start()
    for copy in copies:
        copy.wait()


VMEM = 67043328
IN_VMEM = pl.BlockSpec(memory_space=pltpu.VMEM)
IN_HBM = pl.BlockSpec(memory_space=pltpu.HBM)


def call(kernel, name, far, near, outs, flops, scratch=(), left=24 << 20, out_spec=IN_VMEM):
    inputs = (*far, *near)
    moved = sum(a.size * a.dtype.itemsize for a in (*inputs, *outs))
    results = pl.pallas_call(
        kernel,
        name=name,
        out_shape=outs,
        in_specs=[IN_HBM] * len(far) + [IN_VMEM] * len(near),
        out_specs=[out_spec] * len(outs),
        scratch_shapes=list(scratch),
        compiler_params=pltpu.CompilerParams(vmem_limit_bytes=VMEM - left),
        cost_estimate=pl.CostEstimate(flops=flops, bytes_accessed=moved, transcendentals=0),
    )(*inputs)
    return results if len(outs) > 1 else results[0]


def body(
    probe_preactivation,
    retention_preactivation,
    source_entries,
    extra_log_retention,
    retention_slack,
    group_normalizer_gain,
    readout_mapping_matrix,
):
    tokens, channels = probe_preactivation.shape
    heads = channels // HEAD
    positions = lax.axis_size(SP)
    slabs = positions // heads
    rows = HEAD // slabs
    width = readout_mapping_matrix.shape[1]
    slack = retention_slack.reshape(1, channels)
    gain = group_normalizer_gain.reshape(1, HEAD)
    extra = extra_log_retention.T
    flops = 2 * tokens * channels * HEAD
    inputs = (retention_preactivation, extra, slack, source_entries)

    def near(arrays):
        return (
            tuple(pltpu.VMEM(a.shape, a.dtype) for a in arrays),
            pltpu.SemaphoreType.DMA((len(arrays),)),
        )

    message = call(
        lambda *refs: state_kernel(slabs, refs[:4], *refs[4:]),
        "state",
        inputs,
        (),
        [jax.ShapeDtypeStruct((positions, rows // 2 + 1, 2, HEAD), BF16)],
        4 * flops,
        near(inputs),
        0,
    )
    arrived = lax.all_to_all(message, SP, split_axis=0, concat_axis=0, tiled=True)
    inputs = (*inputs, probe_preactivation)
    inside, reading = call(
        lambda *refs: local_kernel(refs[:5], *refs[5:]),
        "local",
        inputs,
        (),
        [jax.ShapeDtypeStruct((tokens, channels), BF16)] * 2,
        6 * flops,
        near(inputs),
        10300000,
    )
    arrived, inside, reading = lax.optimization_barrier((arrived, inside, reading))
    scanned = call(
        functools.partial(scan_kernel, slabs),
        "scan",
        (),
        (arrived,),
        [jax.ShapeDtypeStruct((positions, rows, HEAD), BF16)],
        40 * flops,
        [pltpu.VMEM((HEAD, positions), F32)],
    )
    entering = lax.all_to_all(scanned, SP, split_axis=0, concat_axis=0, tiled=True)
    entering = entering.reshape(heads, HEAD, HEAD)
    half = tokens // lax.axis_size("tp")

    def projected(away, dtype):
        return call(
            functools.partial(output_kernel, away),
            "away" if away else "kept",
            (),
            (inside, reading, entering, gain, readout_mapping_matrix),
            [jax.ShapeDtypeStruct((half, width), dtype)],
            half * channels * width * 2,
            [pltpu.VMEM((half, channels), BF16)],
        )

    received = lax.ppermute(projected(True, BF16), "tp", [(0, 1), (1, 0)])
    pieces = 4
    return call(
        final_kernel,
        "final",
        (),
        (projected(False, F32), received),
        [jax.ShapeDtypeStruct((half, width), BF16)],
        half * width,
        [pltpu.VMEM((pieces, half // pieces, width), BF16), pltpu.SemaphoreType.DMA((pieces,))],
        out_spec=IN_HBM,
    )


def solution(mesh):
    finer = Mesh(
        mesh.devices.reshape(mesh.shape["grp"], 8, 8, mesh.shape["tp"]),
        ("grp", "sp_0", "sp_1", "tp"),
    )
    in_specs = (
        P(GRP_SP, "tp"),
        P(GRP_SP, "tp"),
        P(GRP_SP, "tp"),
        P(GRP_SP, "tp"),
        P("tp"),
        P(),
        P("tp", None),
    )
    out_specs = P(GRP_SP_TP, None)
    return jax.shard_map(body, mesh=finer, in_specs=in_specs, out_specs=out_specs, check_vma=False)
```

```python
import functools

import jax
import jax.numpy as jnp
from jax import lax
from jax.experimental import pallas as pl
from jax.experimental.pallas import tpu as pltpu
from jax.sharding import Mesh
from jax.sharding import PartitionSpec as P

SPAN = 128
HEAD = 128
SP = ("sp_0", "sp_1")
GRP_SP = ("grp", "sp_0", "sp_1")
GRP_SP_TP = ("grp", "sp_0", "sp_1", "tp")
F32 = jnp.float32
BF16 = jnp.bfloat16


def dot(a, b, contract):
    return lax.dot_general(a, b, (contract, ((), ())), preferred_element_type=F32)


def two_parts(x):
    high = x.astype(BF16)
    return high, (x - high.astype(F32)).astype(BF16)


def summed_rows(selection, x):
    return sum(dot(selection, part, ((1,), (0,))) for part in two_parts(x))


def keyed_and_log_decay(retention, slack, extra):
    keyed = slack * jax.nn.sigmoid(-retention.astype(F32))
    return keyed, jnp.log(1.0 - keyed) + extra


def rows_and_columns(shape):
    return lax.broadcasted_iota(jnp.int32, shape, 0), lax.broadcasted_iota(jnp.int32, shape, 1)


def for_pair(by_token, p):
    return jnp.concatenate(
        [
            jnp.broadcast_to(by_token[:, h : h + 1], (by_token.shape[0], HEAD))
            for h in (2 * p, 2 * p + 1)
        ],
        axis=1,
    )


def copied(pairs, sems):
    copies = [pltpu.make_async_copy(a, b, sems.at[i]) for i, (a, b) in enumerate(pairs)]
    for copy in copies:
        copy.start()
    return copies


def staggered(make, count):
    chains = [make(i) for i in range(count)]
    live = []
    while chains or live:
        if chains:
            live.append(chains.pop(0))
        live = [chain for chain in live if next(chain, live) is None]


def state_kernel(slabs, far, far_message, near, sems, message, out_sems):
    copies = copied(zip(far, near), sems)
    leaving = []
    retention, extra, slack, source = near
    tokens, channels = retention.shape
    wide = 2 * HEAD
    rows = HEAD // slabs
    r, c = rows_and_columns((tokens, tokens))
    later = (c > r).astype(BF16)
    for copy in copies[:-1]:
        copy.wait()
    by_token = extra[...].T

    def chain(p):
        lanes = slice(p * wide, (p + 1) * wide)
        keyed, log_decay = keyed_and_log_decay(
            retention[:, lanes], slack[:, lanes], for_pair(by_token, p)
        )
        yield
        ahead = summed_rows(later, log_decay)
        yield
        sent = (keyed * jnp.exp(ahead)).astype(BF16)
        total = ahead[:1] + log_decay[:1]
        parts = jnp.concatenate(two_parts(total), axis=0)
        yield
        if p == 0:
            copies[-1].wait()
        for k in range(2):
            part = slice(k * HEAD, (k + 1) * HEAD)
            h = 2 * p + k
            values = source[:, h * HEAD : (h + 1) * HEAD]
            state = dot(sent[:, part], values, ((0,), (0,)))
            message[h * slabs : (h + 1) * slabs, : rows // 2] = state.astype(BF16).reshape(
                slabs, rows // 2, 2, HEAD
            )
            message[h * slabs : (h + 1) * slabs, rows // 2] = jnp.broadcast_to(
                parts[None, :, part], (slabs, 2, HEAD)
            )
        yield
        owners = slice(2 * p * slabs, 2 * (p + 1) * slabs)
        leaving.append(
            pltpu.make_async_copy(message.at[owners], far_message.at[owners], out_sems.at[p])
        )
        leaving[-1].start()

    staggered(chain, channels // wide)
    for copy in leaving:
        copy.wait()


def scan_kernel(slabs, message, entering, by_channel):
    positions, rows, _ = entering.shape
    slab = lax.rem(lax.axis_index(SP), slabs)
    parts = message[:, rows // 2].astype(F32)
    by_channel[...] = jnp.exp(parts[:, 0] + parts[:, 1]).T
    mine = by_channel[pl.ds(pl.multiple_of(slab * rows, rows), rows), :]
    state = jnp.zeros((rows, HEAD), F32)
    for i in range(positions):
        entering[i] = state.astype(BF16)
        if i + 1 < positions:
            state = mine[:, i : i + 1] * state + message[i, : rows // 2].astype(F32).reshape(rows, HEAD)


def local_kernel(far, far_inside, far_reading, near, sems, inside, reading, out_sems):
    copies = copied(zip(far, near), sems)
    leaving = []
    retention, extra, slack, source, probe = near
    tokens, channels = retention.shape
    wide = 2 * HEAD
    r, c = rows_and_columns((tokens, tokens))
    within = ((c <= r) & (r // SPAN == c // SPAN)).astype(BF16)
    r, c = rows_and_columns((SPAN, SPAN))
    upto = c <= r
    for copy in copies:
        copy.wait()
    by_token = extra[...].T

    def chain(p):
        lanes = slice(p * wide, (p + 1) * wide)
        keyed, log_decay = keyed_and_log_decay(
            retention[:, lanes], slack[:, lanes], for_pair(by_token, p)
        )
        yield
        running = summed_rows(within, log_decay)
        yield
        raised = jax.nn.silu(probe[:, lanes].astype(F32)) * jnp.exp(running)
        lifted = raised.astype(BF16)
        lowered = (keyed * jnp.exp(-running)).astype(BF16)
        yield
        decayed, before = None, [None, None]
        for b in range(tokens // SPAN):
            span = slice(b * SPAN, (b + 1) * SPAN)
            last = running[(b + 1) * SPAN - 1 : (b + 1) * SPAN]
            if b == 0:
                reading[span, lanes] = lifted[span]
            else:
                reading[span, lanes] = (raised[span] * jnp.exp(decayed)).astype(BF16)
            more = (b + 1) * SPAN < tokens
            if more:
                sent = (keyed[span] * jnp.exp(last - running[span])).astype(BF16)
                decayed = last if b == 0 else decayed + last
            weights = []
            for k in range(2):
                part = slice(k * HEAD, (k + 1) * HEAD)
                scores = dot(lifted[span, part], lowered[span, part], ((1,), (1,)))
                weights.append(jnp.where(upto, scores, 0.0).astype(BF16))
            yield
            for k in range(2):
                part = slice(k * HEAD, (k + 1) * HEAD)
                columns = slice(p * wide + k * HEAD, p * wide + (k + 1) * HEAD)
                values = source[span, columns]
                left, right = weights[k], values
                if b > 0:
                    left = jnp.concatenate([left, lifted[span, part]], axis=1)
                    right = jnp.concatenate([right, before[k].astype(BF16)], axis=0)
                inside[span, columns] = dot(left, right, ((1,), (0,))).astype(BF16)
                if more:
                    added = dot(sent[:, part], values, ((0,), (0,)))
                    if b > 0:
                        added = jnp.exp(last[:, part]).reshape(HEAD, 1) * before[k] + added
                    before[k] = added
            yield
        for i, (a, b) in enumerate(((inside, far_inside), (reading, far_reading))):
            leaving.append(
                pltpu.make_async_copy(a.at[:, lanes], b.at[:, lanes], out_sems.at[i, p])
            )
            leaving[-1].start()

    staggered(chain, channels // wide)
    for copy in leaving:
        copy.wait()


def output_kernel(away, inside, reading, entering, gain, matrix, out, normed):
    tokens = out.shape[0]
    mine = lax.axis_index("tp")
    half = 1 - mine if away else mine
    rows = pl.ds(pl.multiple_of(half * tokens, tokens), tokens)
    for h in range(entering.shape[0]):
        lanes = slice(h * HEAD, (h + 1) * HEAD)
        mixer = inside[rows, lanes] + dot(reading[rows, lanes], entering[h], ((1,), (0,)))
        scale = lax.rsqrt(jnp.mean(mixer * mixer, axis=-1, keepdims=True) + 1e-06)
        normed[:, lanes] = (mixer * scale * gain[...]).astype(BF16)
    out[...] = dot(normed[...], matrix[...], ((1,), (0,))).astype(out.dtype)


def final_kernel(kept, received, far, out, sems):
    pieces, rows, _ = out.shape
    copies = []
    for i in range(pieces):
        span = slice(i * rows, (i + 1) * rows)
        out[i] = (kept[span] + received[span].astype(F32)).astype(BF16)
        copies.append(pltpu.make_async_copy(out.at[i], far.at[span], sems.at[i]))
        if i > 0:
            copies[i - 1].start()
    copies[-1].start()
    for copy in copies:
        copy.wait()


VMEM = 67043328
IN_VMEM = pl.BlockSpec(memory_space=pltpu.VMEM)
IN_HBM = pl.BlockSpec(memory_space=pltpu.HBM)


def call(kernel, name, far, near, outs, flops, scratch=(), left=24 << 20, out_spec=IN_VMEM):
    inputs = (*far, *near)
    moved = sum(a.size * a.dtype.itemsize for a in (*inputs, *outs))
    results = pl.pallas_call(
        kernel,
        name=name,
        out_shape=outs,
        in_specs=[IN_HBM] * len(far) + [IN_VMEM] * len(near),
        out_specs=[out_spec] * len(outs),
        scratch_shapes=list(scratch),
        compiler_params=pltpu.CompilerParams(vmem_limit_bytes=VMEM - left),
        cost_estimate=pl.CostEstimate(flops=flops, bytes_accessed=moved, transcendentals=0),
    )(*inputs)
    return results if len(outs) > 1 else results[0]


def body(
    probe_preactivation,
    retention_preactivation,
    source_entries,
    extra_log_retention,
    retention_slack,
    group_normalizer_gain,
    readout_mapping_matrix,
):
    tokens, channels = probe_preactivation.shape
    heads = channels // HEAD
    positions = lax.axis_size(SP)
    slabs = positions // heads
    rows = HEAD // slabs
    width = readout_mapping_matrix.shape[1]
    slack = retention_slack.reshape(1, channels)
    gain = group_normalizer_gain.reshape(1, HEAD)
    extra = extra_log_retention.T
    flops = 2 * tokens * channels * HEAD
    inputs = (retention_preactivation, extra, slack, source_entries)

    def near(arrays):
        return (
            tuple(pltpu.VMEM(a.shape, a.dtype) for a in arrays),
            pltpu.SemaphoreType.DMA((len(arrays),)),
        )

    message = call(
        lambda *refs: state_kernel(slabs, refs[:4], *refs[4:]),
        "state",
        inputs,
        (),
        [jax.ShapeDtypeStruct((positions, rows // 2 + 1, 2, HEAD), BF16)],
        4 * flops,
        (
            *near(inputs),
            pltpu.VMEM((positions, rows // 2 + 1, 2, HEAD), BF16),
            pltpu.SemaphoreType.DMA((channels // (2 * HEAD),)),
        ),
        0,
        IN_HBM,
    )
    arrived = lax.all_to_all(message, SP, split_axis=0, concat_axis=0, tiled=True)
    inputs = (*inputs, probe_preactivation)
    inside, reading = call(
        lambda *refs: local_kernel(refs[:5], *refs[5:]),
        "local",
        inputs,
        (),
        [jax.ShapeDtypeStruct((tokens, channels), BF16)] * 2,
        6 * flops,
        (
            *near(inputs),
            *[pltpu.VMEM((tokens, channels), BF16)] * 2,
            pltpu.SemaphoreType.DMA((2, channels // (2 * HEAD))),
        ),
        10300000,
        IN_HBM,
    )
    arrived, inside, reading = lax.optimization_barrier((arrived, inside, reading))
    scanned = call(
        functools.partial(scan_kernel, slabs),
        "scan",
        (),
        (arrived,),
        [jax.ShapeDtypeStruct((positions, rows, HEAD), BF16)],
        40 * flops,
        [pltpu.VMEM((HEAD, positions), F32)],
    )
    entering = lax.all_to_all(scanned, SP, split_axis=0, concat_axis=0, tiled=True)
    entering = entering.reshape(heads, HEAD, HEAD)
    half = tokens // lax.axis_size("tp")

    def projected(away, dtype):
        return call(
            functools.partial(output_kernel, away),
            "away" if away else "kept",
            (),
            (inside, reading, entering, gain, readout_mapping_matrix),
            [jax.ShapeDtypeStruct((half, width), dtype)],
            half * channels * width * 2,
            [pltpu.VMEM((half, channels), BF16)],
        )

    received = lax.ppermute(projected(True, BF16), "tp", [(0, 1), (1, 0)])
    pieces = 4
    return call(
        final_kernel,
        "final",
        (),
        (projected(False, F32), received),
        [jax.ShapeDtypeStruct((half, width), BF16)],
        half * width,
        [pltpu.VMEM((pieces, half // pieces, width), BF16), pltpu.SemaphoreType.DMA((pieces,))],
        out_spec=IN_HBM,
    )


def solution(mesh):
    finer = Mesh(
        mesh.devices.reshape(mesh.shape["grp"], 8, 8, mesh.shape["tp"]),
        ("grp", "sp_0", "sp_1", "tp"),
    )
    in_specs = (
        P(GRP_SP, "tp"),
        P(GRP_SP, "tp"),
        P(GRP_SP, "tp"),
        P(GRP_SP, "tp"),
        P("tp"),
        P(),
        P("tp", None),
    )
    out_specs = P(GRP_SP_TP, None)
    return jax.shard_map(body, mesh=finer, in_specs=in_specs, out_specs=out_specs, check_vma=False)
```

```python
import functools

import jax
import jax.numpy as jnp
from jax import lax
from jax.experimental import pallas as pl
from jax.experimental.pallas import tpu as pltpu
from jax.sharding import Mesh
from jax.sharding import PartitionSpec as P

SPAN = 128
HEAD = 128
SP = ("sp_0", "sp_1")
GRP_SP = ("grp", "sp_0", "sp_1")
GRP_SP_TP = ("grp", "sp_0", "sp_1", "tp")
F32 = jnp.float32
BF16 = jnp.bfloat16


def dot(a, b, contract):
    return lax.dot_general(a, b, (contract, ((), ())), preferred_element_type=F32)


def two_parts(x):
    high = x.astype(BF16)
    return high, (x - high.astype(F32)).astype(BF16)


def summed_rows(selection, x):
    return sum(dot(selection, part, ((1,), (0,))) for part in two_parts(x))


def keyed_and_log_decay(retention, slack, extra):
    keyed = slack * jax.nn.sigmoid(-retention.astype(F32))
    return keyed, jnp.log(1.0 - keyed) + extra


def rows_and_columns(shape):
    return lax.broadcasted_iota(jnp.int32, shape, 0), lax.broadcasted_iota(jnp.int32, shape, 1)


def for_pair(by_token, p):
    return jnp.concatenate(
        [
            jnp.broadcast_to(by_token[:, h : h + 1], (by_token.shape[0], HEAD))
            for h in (2 * p, 2 * p + 1)
        ],
        axis=1,
    )


def copied(pairs, sems):
    copies = [pltpu.make_async_copy(a, b, sems.at[i]) for i, (a, b) in enumerate(pairs)]
    for copy in copies:
        copy.start()
    return copies


def staggered(make, count):
    chains = [make(i) for i in range(count)]
    live = []
    while chains or live:
        if chains:
            live.append(chains.pop(0))
        live = [chain for chain in live if next(chain, live) is None]


def state_kernel(slabs, far, message, near, sems):
    copies = copied(zip(far, near), sems)
    retention, extra, slack, source = near
    tokens, channels = retention.shape
    wide = 2 * HEAD
    rows = HEAD // slabs
    r, c = rows_and_columns((tokens, tokens))
    later = (c > r).astype(BF16)
    for copy in copies:
        copy.wait()
    by_token = extra[...].T

    def chain(p):
        lanes = slice(p * wide, (p + 1) * wide)
        added = for_pair(by_token, p)
        halves = []
        for q in range(2):
            span = slice(q * tokens // 2, (q + 1) * tokens // 2)
            halves.append(
                keyed_and_log_decay(retention[span, lanes], slack[:, lanes], added[span])
            )
            yield
        log_decay = jnp.concatenate([x[1] for x in halves], axis=0)
        high, low = two_parts(log_decay)
        ahead = []
        for q in range(2):
            part = later[q * tokens // 2 : (q + 1) * tokens // 2]
            ahead.append(dot(part, high, ((1,), (0,))) + dot(part, low, ((1,), (0,))))
            yield
        sent = jnp.concatenate(
            [(halves[q][0] * jnp.exp(ahead[q])).astype(BF16) for q in range(2)], axis=0
        )
        total = ahead[0][:1] + log_decay[:1]
        parts = jnp.concatenate(two_parts(total), axis=0)
        yield
        for k in range(2):
            part = slice(k * HEAD, (k + 1) * HEAD)
            h = 2 * p + k
            values = source[:, h * HEAD : (h + 1) * HEAD]
            state = dot(sent[:, part], values, ((0,), (0,)))
            message[h * slabs : (h + 1) * slabs, : rows // 2] = state.astype(BF16).reshape(
                slabs, rows // 2, 2, HEAD
            )
            message[h * slabs : (h + 1) * slabs, rows // 2] = jnp.broadcast_to(
                parts[None, :, part], (slabs, 2, HEAD)
            )

    staggered(chain, channels // wide)


def scan_kernel(slabs, message, entering, by_channel):
    positions, rows, _ = entering.shape
    slab = lax.rem(lax.axis_index(SP), slabs)
    r, c = rows_and_columns((2 * positions, positions))
    pairs = (r // 2 == c).astype(BF16)
    decays = message[:, rows // 2].reshape(2 * positions, HEAD)
    by_channel[...] = dot(decays, pairs, ((0,), (0,)))
    mine = jnp.exp(by_channel[pl.ds(pl.multiple_of(slab * rows, rows), rows), :])
    state = jnp.zeros((rows, HEAD), F32)
    for i in range(positions):
        entering[i] = state.astype(BF16)
        if i + 1 < positions:
            state = mine[:, i : i + 1] * state + message[i, : rows // 2].astype(F32).reshape(rows, HEAD)


def local_kernel(far, inside, reading, near, sems):
    copies = copied(zip(far, near), sems)
    retention, extra, slack, source, probe = near
    tokens, channels = retention.shape
    wide = 2 * HEAD
    r, c = rows_and_columns((tokens, tokens))
    within = ((c <= r) & (r // SPAN == c // SPAN)).astype(BF16)
    r, c = rows_and_columns((SPAN, SPAN))
    upto = c <= r
    for copy in copies:
        copy.wait()
    by_token = extra[...].T

    def chain(p):
        lanes = slice(p * wide, (p + 1) * wide)
        keyed, log_decay = keyed_and_log_decay(
            retention[:, lanes], slack[:, lanes], for_pair(by_token, p)
        )
        yield
        running = summed_rows(within, log_decay)
        yield
        raised = jax.nn.silu(probe[:, lanes].astype(F32)) * jnp.exp(running)
        lifted = raised.astype(BF16)
        lowered = (keyed * jnp.exp(-running)).astype(BF16)
        yield
        decayed, before = None, [None, None]
        for b in range(tokens // SPAN):
            span = slice(b * SPAN, (b + 1) * SPAN)
            last = running[(b + 1) * SPAN - 1 : (b + 1) * SPAN]
            if b == 0:
                reading[span, lanes] = lifted[span]
            else:
                reading[span, lanes] = (raised[span] * jnp.exp(decayed)).astype(BF16)
            more = (b + 1) * SPAN < tokens
            if more:
                sent = (keyed[span] * jnp.exp(last - running[span])).astype(BF16)
                decayed = last if b == 0 else decayed + last
            weights = []
            for k in range(2):
                part = slice(k * HEAD, (k + 1) * HEAD)
                scores = dot(lifted[span, part], lowered[span, part], ((1,), (1,)))
                weights.append(jnp.where(upto, scores, 0.0).astype(BF16))
            yield
            for k in range(2):
                part = slice(k * HEAD, (k + 1) * HEAD)
                columns = slice(p * wide + k * HEAD, p * wide + (k + 1) * HEAD)
                values = source[span, columns]
                left, right = weights[k], values
                if b > 0:
                    left = jnp.concatenate([left, lifted[span, part]], axis=1)
                    right = jnp.concatenate([right, before[k].astype(BF16)], axis=0)
                inside[span, columns] = dot(left, right, ((1,), (0,))).astype(BF16)
                if more:
                    added = dot(sent[:, part], values, ((0,), (0,)))
                    if b > 0:
                        added = jnp.exp(last[:, part]).reshape(HEAD, 1) * before[k] + added
                    before[k] = added
            yield

    staggered(chain, channels // wide)


def output_kernel(away, inside, reading, entering, gain, matrix, out, normed):
    tokens = out.shape[0]
    mine = lax.axis_index("tp")
    half = 1 - mine if away else mine
    rows = pl.ds(pl.multiple_of(half * tokens, tokens), tokens)
    for h in range(entering.shape[0]):
        lanes = slice(h * HEAD, (h + 1) * HEAD)
        mixer = inside[rows, lanes] + dot(reading[rows, lanes], entering[h], ((1,), (0,)))
        scale = lax.rsqrt(jnp.mean(mixer * mixer, axis=-1, keepdims=True) + 1e-06)
        normed[:, lanes] = (mixer * scale * gain[...]).astype(BF16)
    out[...] = dot(normed[...], matrix[...], ((1,), (0,))).astype(out.dtype)


def final_kernel(kept, received, far, out, sems):
    pieces, rows, _ = out.shape
    copies = []
    for i in range(pieces):
        span = slice(i * rows, (i + 1) * rows)
        out[i] = (kept[span] + received[span].astype(F32)).astype(BF16)
        copies.append(pltpu.make_async_copy(out.at[i], far.at[span], sems.at[i]))
        copies[-1].start()
    for copy in copies:
        copy.wait()


VMEM = 67043328
IN_VMEM = pl.BlockSpec(memory_space=pltpu.VMEM)
IN_HBM = pl.BlockSpec(memory_space=pltpu.HBM)


def call(kernel, name, far, near, outs, flops, scratch=(), left=24 << 20, out_spec=IN_VMEM):
    inputs = (*far, *near)
    moved = sum(a.size * a.dtype.itemsize for a in (*inputs, *outs))
    results = pl.pallas_call(
        kernel,
        name=name,
        out_shape=outs,
        in_specs=[IN_HBM] * len(far) + [IN_VMEM] * len(near),
        out_specs=[out_spec] * len(outs),
        scratch_shapes=list(scratch),
        compiler_params=pltpu.CompilerParams(vmem_limit_bytes=VMEM - left),
        cost_estimate=pl.CostEstimate(flops=flops, bytes_accessed=moved, transcendentals=0),
    )(*inputs)
    return results if len(outs) > 1 else results[0]


def body(
    probe_preactivation,
    retention_preactivation,
    source_entries,
    extra_log_retention,
    retention_slack,
    group_normalizer_gain,
    readout_mapping_matrix,
):
    tokens, channels = probe_preactivation.shape
    heads = channels // HEAD
    positions = lax.axis_size(SP)
    slabs = positions // heads
    rows = HEAD // slabs
    width = readout_mapping_matrix.shape[1]
    slack = retention_slack.reshape(1, channels)
    gain = group_normalizer_gain.reshape(1, HEAD)
    extra = extra_log_retention.T
    flops = 2 * tokens * channels * HEAD
    inputs = (retention_preactivation, extra, slack, source_entries)

    def near(arrays):
        return (
            tuple(pltpu.VMEM(a.shape, a.dtype) for a in arrays),
            pltpu.SemaphoreType.DMA((len(arrays),)),
        )

    message = call(
        lambda *refs: state_kernel(slabs, refs[:4], *refs[4:]),
        "state",
        inputs,
        (),
        [jax.ShapeDtypeStruct((positions, rows // 2 + 1, 2, HEAD), BF16)],
        4 * flops,
        near(inputs),
        0,
    )
    arrived = lax.all_to_all(message, SP, split_axis=0, concat_axis=0, tiled=True)
    inputs = (*inputs, probe_preactivation)
    inside, reading = call(
        lambda *refs: local_kernel(refs[:5], *refs[5:]),
        "local",
        inputs,
        (),
        [jax.ShapeDtypeStruct((tokens, channels), BF16)] * 2,
        6 * flops,
        near(inputs),
        10300000,
    )
    arrived, inside, reading = lax.optimization_barrier((arrived, inside, reading))
    scanned = call(
        functools.partial(scan_kernel, slabs),
        "scan",
        (),
        (arrived,),
        [jax.ShapeDtypeStruct((positions, rows, HEAD), BF16)],
        40 * flops,
        [pltpu.VMEM((HEAD, positions), F32)],
    )
    entering = lax.all_to_all(scanned, SP, split_axis=0, concat_axis=0, tiled=True)
    entering = entering.reshape(heads, HEAD, HEAD)
    half = tokens // lax.axis_size("tp")

    def projected(away, dtype):
        return call(
            functools.partial(output_kernel, away),
            "away" if away else "kept",
            (),
            (inside, reading, entering, gain, readout_mapping_matrix),
            [jax.ShapeDtypeStruct((half, width), dtype)],
            half * channels * width * 2,
            [pltpu.VMEM((half, channels), BF16)],
        )

    received = lax.ppermute(projected(True, BF16), "tp", [(0, 1), (1, 0)])
    pieces = 4
    return call(
        final_kernel,
        "final",
        (),
        (projected(False, F32), received),
        [jax.ShapeDtypeStruct((half, width), BF16)],
        half * width,
        [pltpu.VMEM((pieces, half // pieces, width), BF16), pltpu.SemaphoreType.DMA((pieces,))],
        out_spec=IN_HBM,
    )


def solution(mesh):
    finer = Mesh(
        mesh.devices.reshape(mesh.shape["grp"], 8, 8, mesh.shape["tp"]),
        ("grp", "sp_0", "sp_1", "tp"),
    )
    in_specs = (
        P(GRP_SP, "tp"),
        P(GRP_SP, "tp"),
        P(GRP_SP, "tp"),
        P(GRP_SP, "tp"),
        P("tp"),
        P(),
        P("tp", None),
    )
    out_specs = P(GRP_SP_TP, None)
    return jax.shard_map(body, mesh=finer, in_specs=in_specs, out_specs=out_specs, check_vma=False)
```

```python
import functools

import jax
import jax.numpy as jnp
from jax import lax
from jax.experimental import pallas as pl
from jax.experimental.pallas import tpu as pltpu
from jax.sharding import Mesh
from jax.sharding import PartitionSpec as P

SPAN = 128
HEAD = 128
SP = ("sp_0", "sp_1")
GRP_SP = ("grp", "sp_0", "sp_1")
GRP_SP_TP = ("grp", "sp_0", "sp_1", "tp")
F32 = jnp.float32
BF16 = jnp.bfloat16


def dot(a, b, contract):
    return lax.dot_general(a, b, (contract, ((), ())), preferred_element_type=F32)


def two_parts(x):
    high = x.astype(BF16)
    return high, (x - high.astype(F32)).astype(BF16)


def summed_rows(selection, x):
    return sum(dot(selection, part, ((1,), (0,))) for part in two_parts(x))


def keyed_and_log_decay(retention, slack, extra):
    keyed = slack * jax.nn.sigmoid(-retention.astype(F32))
    return keyed, jnp.log(1.0 - keyed) + extra


def rows_and_columns(shape):
    return lax.broadcasted_iota(jnp.int32, shape, 0), lax.broadcasted_iota(jnp.int32, shape, 1)


def for_pair(by_token, p):
    return jnp.concatenate(
        [
            jnp.broadcast_to(by_token[:, h : h + 1], (by_token.shape[0], HEAD))
            for h in (2 * p, 2 * p + 1)
        ],
        axis=1,
    )


PIECES = 4


def copied(pairs, sems):
    groups = []
    for i, (source, target) in enumerate(pairs):
        rows = source.shape[0]
        pieces = PIECES if rows % (PIECES * 16) == 0 else 1
        group = []
        for k in range(pieces):
            span = pl.ds(k * (rows // pieces), rows // pieces)
            group.append(
                pltpu.make_async_copy(source.at[span], target.at[span], sems.at[i, k])
            )
            group[-1].start()
        groups.append(group)
    return groups


def wait_all(groups):
    for group in groups:
        for copy in group:
            copy.wait()


def staggered(make, count):
    chains = [make(i) for i in range(count)]
    live = []
    while chains or live:
        if chains:
            live.append(chains.pop(0))
        live = [chain for chain in live if next(chain, live) is None]


def state_kernel(slabs, far, message, near, sems):
    copies = copied(zip(far, near), sems)
    retention, extra, slack, source = near
    tokens, channels = retention.shape
    wide = 2 * HEAD
    rows = HEAD // slabs
    r, c = rows_and_columns((tokens, tokens))
    later = (c > r).astype(BF16)
    wait_all(copies[:-1])
    by_token = extra[...].T

    def chain(p):
        lanes = slice(p * wide, (p + 1) * wide)
        keyed, log_decay = keyed_and_log_decay(
            retention[:, lanes], slack[:, lanes], for_pair(by_token, p)
        )
        yield
        ahead = summed_rows(later, log_decay)
        yield
        sent = (keyed * jnp.exp(ahead)).astype(BF16)
        total = ahead[:1] + log_decay[:1]
        parts = jnp.concatenate(two_parts(total), axis=0)
        yield
        if p == 0:
            wait_all(copies[-1:])
        for k in range(2):
            part = slice(k * HEAD, (k + 1) * HEAD)
            h = 2 * p + k
            values = source[:, h * HEAD : (h + 1) * HEAD]
            state = dot(sent[:, part], values, ((0,), (0,)))
            message[h * slabs : (h + 1) * slabs, : rows // 2] = state.astype(BF16).reshape(
                slabs, rows // 2, 2, HEAD
            )
            message[h * slabs : (h + 1) * slabs, rows // 2] = jnp.broadcast_to(
                parts[None, :, part], (slabs, 2, HEAD)
            )

    staggered(chain, channels // wide)


def scan_kernel(slabs, message, entering, by_channel):
    positions, rows, _ = entering.shape
    slab = lax.rem(lax.axis_index(SP), slabs)
    parts = message[:, rows // 2].astype(F32)
    by_channel[...] = jnp.exp(parts[:, 0] + parts[:, 1]).T
    mine = by_channel[pl.ds(pl.multiple_of(slab * rows, rows), rows), :]
    state = jnp.zeros((rows, HEAD), F32)
    for i in range(positions):
        entering[i] = state.astype(BF16)
        if i + 1 < positions:
            state = mine[:, i : i + 1] * state + message[i, : rows // 2].astype(F32).reshape(rows, HEAD)


def local_kernel(far, inside, reading, near, sems):
    copies = copied(zip(far, near), sems)
    retention, extra, slack, source, probe = near
    tokens, channels = retention.shape
    wide = 2 * HEAD
    r, c = rows_and_columns((tokens, tokens))
    within = ((c <= r) & (r // SPAN == c // SPAN)).astype(BF16)
    r, c = rows_and_columns((SPAN, SPAN))
    upto = c <= r
    wait_all(copies)
    by_token = extra[...].T

    def chain(p):
        lanes = slice(p * wide, (p + 1) * wide)
        keyed, log_decay = keyed_and_log_decay(
            retention[:, lanes], slack[:, lanes], for_pair(by_token, p)
        )
        yield
        running = summed_rows(within, log_decay)
        yield
        raised = jax.nn.silu(probe[:, lanes].astype(F32)) * jnp.exp(running)
        lifted = raised.astype(BF16)
        lowered = (keyed * jnp.exp(-running)).astype(BF16)
        yield
        decayed, before = None, [None, None]
        for b in range(tokens // SPAN):
            span = slice(b * SPAN, (b + 1) * SPAN)
            last = running[(b + 1) * SPAN - 1 : (b + 1) * SPAN]
            if b == 0:
                reading[span, lanes] = lifted[span]
            else:
                reading[span, lanes] = (raised[span] * jnp.exp(decayed)).astype(BF16)
            more = (b + 1) * SPAN < tokens
            if more:
                sent = (keyed[span] * jnp.exp(last - running[span])).astype(BF16)
                decayed = last if b == 0 else decayed + last
            weights = []
            for k in range(2):
                part = slice(k * HEAD, (k + 1) * HEAD)
                scores = dot(lifted[span, part], lowered[span, part], ((1,), (1,)))
                weights.append(jnp.where(upto, scores, 0.0).astype(BF16))
            yield
            for k in range(2):
                part = slice(k * HEAD, (k + 1) * HEAD)
                columns = slice(p * wide + k * HEAD, p * wide + (k + 1) * HEAD)
                values = source[span, columns]
                left, right = weights[k], values
                if b > 0:
                    left = jnp.concatenate([left, lifted[span, part]], axis=1)
                    right = jnp.concatenate([right, before[k].astype(BF16)], axis=0)
                inside[span, columns] = dot(left, right, ((1,), (0,))).astype(BF16)
                if more:
                    added = dot(sent[:, part], values, ((0,), (0,)))
                    if b > 0:
                        added = jnp.exp(last[:, part]).reshape(HEAD, 1) * before[k] + added
                    before[k] = added
            yield

    staggered(chain, channels // wide)


def output_kernel(away, inside, reading, entering, gain, matrix, out, normed):
    tokens = out.shape[0]
    mine = lax.axis_index("tp")
    half = 1 - mine if away else mine
    rows = pl.ds(pl.multiple_of(half * tokens, tokens), tokens)
    for h in range(entering.shape[0]):
        lanes = slice(h * HEAD, (h + 1) * HEAD)
        mixer = inside[rows, lanes] + dot(reading[rows, lanes], entering[h], ((1,), (0,)))
        scale = lax.rsqrt(jnp.mean(mixer * mixer, axis=-1, keepdims=True) + 1e-06)
        normed[:, lanes] = (mixer * scale * gain[...]).astype(BF16)
    out[...] = dot(normed[...], matrix[...], ((1,), (0,))).astype(out.dtype)


def final_kernel(kept, received, far, out, sems):
    pieces, rows, _ = out.shape
    copies = []
    for i in range(pieces):
        span = slice(i * rows, (i + 1) * rows)
        out[i] = (kept[span] + received[span].astype(F32)).astype(BF16)
        copies.append(pltpu.make_async_copy(out.at[i], far.at[span], sems.at[i]))
        copies[-1].start()
    for copy in copies:
        copy.wait()


VMEM = 67043328
IN_VMEM = pl.BlockSpec(memory_space=pltpu.VMEM)
IN_HBM = pl.BlockSpec(memory_space=pltpu.HBM)


def call(kernel, name, far, near, outs, flops, scratch=(), left=24 << 20, out_spec=IN_VMEM):
    inputs = (*far, *near)
    moved = sum(a.size * a.dtype.itemsize for a in (*inputs, *outs))
    results = pl.pallas_call(
        kernel,
        name=name,
        out_shape=outs,
        in_specs=[IN_HBM] * len(far) + [IN_VMEM] * len(near),
        out_specs=[out_spec] * len(outs),
        scratch_shapes=list(scratch),
        compiler_params=pltpu.CompilerParams(vmem_limit_bytes=VMEM - left),
        cost_estimate=pl.CostEstimate(flops=flops, bytes_accessed=moved, transcendentals=0),
    )(*inputs)
    return results if len(outs) > 1 else results[0]


def body(
    probe_preactivation,
    retention_preactivation,
    source_entries,
    extra_log_retention,
    retention_slack,
    group_normalizer_gain,
    readout_mapping_matrix,
):
    tokens, channels = probe_preactivation.shape
    heads = channels // HEAD
    positions = lax.axis_size(SP)
    slabs = positions // heads
    rows = HEAD // slabs
    width = readout_mapping_matrix.shape[1]
    slack = retention_slack.reshape(1, channels)
    gain = group_normalizer_gain.reshape(1, HEAD)
    extra = extra_log_retention.T
    flops = 2 * tokens * channels * HEAD
    inputs = (retention_preactivation, extra, slack, source_entries)

    def near(arrays):
        return (
            tuple(pltpu.VMEM(a.shape, a.dtype) for a in arrays),
            pltpu.SemaphoreType.DMA((len(arrays), PIECES)),
        )

    message = call(
        lambda *refs: state_kernel(slabs, refs[:4], *refs[4:]),
        "state",
        inputs,
        (),
        [jax.ShapeDtypeStruct((positions, rows // 2 + 1, 2, HEAD), BF16)],
        4 * flops,
        near(inputs),
        0,
    )
    arrived = lax.all_to_all(message, SP, split_axis=0, concat_axis=0, tiled=True)
    inputs = (*inputs, probe_preactivation)
    inside, reading = call(
        lambda *refs: local_kernel(refs[:5], *refs[5:]),
        "local",
        inputs,
        (),
        [jax.ShapeDtypeStruct((tokens, channels), BF16)] * 2,
        6 * flops,
        near(inputs),
        10300000,
    )
    arrived, inside, reading = lax.optimization_barrier((arrived, inside, reading))
    scanned = call(
        functools.partial(scan_kernel, slabs),
        "scan",
        (),
        (arrived,),
        [jax.ShapeDtypeStruct((positions, rows, HEAD), BF16)],
        40 * flops,
        [pltpu.VMEM((HEAD, positions), F32)],
    )
    entering = lax.all_to_all(scanned, SP, split_axis=0, concat_axis=0, tiled=True)
    entering = entering.reshape(heads, HEAD, HEAD)
    half = tokens // lax.axis_size("tp")

    def projected(away, dtype):
        return call(
            functools.partial(output_kernel, away),
            "away" if away else "kept",
            (),
            (inside, reading, entering, gain, readout_mapping_matrix),
            [jax.ShapeDtypeStruct((half, width), dtype)],
            half * channels * width * 2,
            [pltpu.VMEM((half, channels), BF16)],
        )

    received = lax.ppermute(projected(True, BF16), "tp", [(0, 1), (1, 0)])
    pieces = 4
    return call(
        final_kernel,
        "final",
        (),
        (projected(False, F32), received),
        [jax.ShapeDtypeStruct((half, width), BF16)],
        half * width,
        [pltpu.VMEM((pieces, half // pieces, width), BF16), pltpu.SemaphoreType.DMA((pieces,))],
        out_spec=IN_HBM,
    )


def solution(mesh):
    finer = Mesh(
        mesh.devices.reshape(mesh.shape["grp"], 8, 8, mesh.shape["tp"]),
        ("grp", "sp_0", "sp_1", "tp"),
    )
    in_specs = (
        P(GRP_SP, "tp"),
        P(GRP_SP, "tp"),
        P(GRP_SP, "tp"),
        P(GRP_SP, "tp"),
        P("tp"),
        P(),
        P("tp", None),
    )
    out_specs = P(GRP_SP_TP, None)
    return jax.shard_map(body, mesh=finer, in_specs=in_specs, out_specs=out_specs, check_vma=False)
```

```python
import functools

import jax
import jax.numpy as jnp
from jax import lax
from jax.experimental import pallas as pl
from jax.experimental.pallas import tpu as pltpu
from jax.sharding import PartitionSpec as P

SPAN = 128
HEAD = 128
SP = "sp"
GRP_SP = ("grp", "sp")
GRP_SP_TP = ("grp", "sp", "tp")
F32 = jnp.float32
BF16 = jnp.bfloat16


def dot(a, b, contract):
    return lax.dot_general(a, b, (contract, ((), ())), preferred_element_type=F32)


def two_parts(x):
    high = x.astype(BF16)
    return high, (x - high.astype(F32)).astype(BF16)


def summed_rows(selection, x):
    return sum(dot(selection, part, ((1,), (0,))) for part in two_parts(x))


def keyed_and_log_decay(retention, slack, extra):
    keyed = slack * jax.nn.sigmoid(-retention.astype(F32))
    return keyed, jnp.log(1.0 - keyed) + extra


def rows_and_columns(shape):
    return lax.broadcasted_iota(jnp.int32, shape, 0), lax.broadcasted_iota(jnp.int32, shape, 1)


def for_pair(by_token, p):
    return jnp.concatenate(
        [
            jnp.broadcast_to(by_token[:, h : h + 1], (by_token.shape[0], HEAD))
            for h in (2 * p, 2 * p + 1)
        ],
        axis=1,
    )


def copied(pairs, sems):
    copies = [pltpu.make_async_copy(a, b, sems.at[i]) for i, (a, b) in enumerate(pairs)]
    for copy in copies:
        copy.start()
    return copies


def staggered(make, count):
    chains = [make(i) for i in range(count)]
    live = []
    while chains or live:
        if chains:
            live.append(chains.pop(0))
        live = [chain for chain in live if next(chain, live) is None]


def state_kernel(slabs, far, message, near, sems):
    copies = copied(zip(far, near), sems)
    retention, extra, slack, source = near
    tokens, channels = retention.shape
    wide = 2 * HEAD
    rows = HEAD // slabs
    r, c = rows_and_columns((tokens, tokens))
    later = (c > r).astype(BF16)
    for copy in copies[:-1]:
        copy.wait()
    by_token = extra[...].T

    def chain(p):
        lanes = slice(p * wide, (p + 1) * wide)
        keyed, log_decay = keyed_and_log_decay(
            retention[:, lanes], slack[:, lanes], for_pair(by_token, p)
        )
        yield
        ahead = summed_rows(later, log_decay)
        yield
        sent = (keyed * jnp.exp(ahead)).astype(BF16)
        total = ahead[:1] + log_decay[:1]
        parts = jnp.concatenate(two_parts(total), axis=0)
        yield
        if p == 0:
            copies[-1].wait()
        for k in range(2):
            part = slice(k * HEAD, (k + 1) * HEAD)
            h = 2 * p + k
            values = source[:, h * HEAD : (h + 1) * HEAD]
            state = dot(sent[:, part], values, ((0,), (0,)))
            message[h * slabs : (h + 1) * slabs, : rows // 2] = state.astype(BF16).reshape(
                slabs, rows // 2, 2, HEAD
            )
            message[h * slabs : (h + 1) * slabs, rows // 2] = jnp.broadcast_to(
                parts[None, :, part], (slabs, 2, HEAD)
            )

    staggered(chain, channels // wide)


def scan_kernel(slabs, message, entering, by_channel):
    positions, rows, _ = entering.shape
    slab = lax.rem(lax.axis_index(SP), slabs)
    parts = message[:, rows // 2].astype(F32)
    by_channel[...] = jnp.exp(parts[:, 0] + parts[:, 1]).T
    mine = by_channel[pl.ds(pl.multiple_of(slab * rows, rows), rows), :]
    state = jnp.zeros((rows, HEAD), F32)
    for i in range(positions):
        entering[i] = state.astype(BF16)
        if i + 1 < positions:
            state = mine[:, i : i + 1] * state + message[i, : rows // 2].astype(F32).reshape(rows, HEAD)


def local_kernel(far, inside, reading, near, sems):
    copies = copied(zip(far, near), sems)
    retention, extra, slack, source, probe = near
    tokens, channels = retention.shape
    wide = 2 * HEAD
    r, c = rows_and_columns((tokens, tokens))
    within = ((c <= r) & (r // SPAN == c // SPAN)).astype(BF16)
    r, c = rows_and_columns((SPAN, SPAN))
    upto = c <= r
    for copy in copies:
        copy.wait()
    by_token = extra[...].T

    def chain(p):
        lanes = slice(p * wide, (p + 1) * wide)
        keyed, log_decay = keyed_and_log_decay(
            retention[:, lanes], slack[:, lanes], for_pair(by_token, p)
        )
        yield
        running = summed_rows(within, log_decay)
        yield
        raised = jax.nn.silu(probe[:, lanes].astype(F32)) * jnp.exp(running)
        lifted = raised.astype(BF16)
        lowered = (keyed * jnp.exp(-running)).astype(BF16)
        yield
        decayed, before = None, [None, None]
        for b in range(tokens // SPAN):
            span = slice(b * SPAN, (b + 1) * SPAN)
            last = running[(b + 1) * SPAN - 1 : (b + 1) * SPAN]
            if b == 0:
                reading[span, lanes] = lifted[span]
            else:
                reading[span, lanes] = (raised[span] * jnp.exp(decayed)).astype(BF16)
            more = (b + 1) * SPAN < tokens
            if more:
                sent = (keyed[span] * jnp.exp(last - running[span])).astype(BF16)
                decayed = last if b == 0 else decayed + last
            weights = []
            for k in range(2):
                part = slice(k * HEAD, (k + 1) * HEAD)
                scores = dot(lifted[span, part], lowered[span, part], ((1,), (1,)))
                weights.append(jnp.where(upto, scores, 0.0).astype(BF16))
            yield
            for k in range(2):
                part = slice(k * HEAD, (k + 1) * HEAD)
                columns = slice(p * wide + k * HEAD, p * wide + (k + 1) * HEAD)
                values = source[span, columns]
                left, right = weights[k], values
                if b > 0:
                    left = jnp.concatenate([left, lifted[span, part]], axis=1)
                    right = jnp.concatenate([right, before[k].astype(BF16)], axis=0)
                inside[span, columns] = dot(left, right, ((1,), (0,))).astype(BF16)
                if more:
                    added = dot(sent[:, part], values, ((0,), (0,)))
                    if b > 0:
                        added = jnp.exp(last[:, part]).reshape(HEAD, 1) * before[k] + added
                    before[k] = added
            yield

    staggered(chain, channels // wide)


def output_kernel(away, inside, reading, entering, gain, matrix, out, normed):
    tokens = out.shape[0]
    mine = lax.axis_index("tp")
    half = 1 - mine if away else mine
    rows = pl.ds(pl.multiple_of(half * tokens, tokens), tokens)
    for h in range(entering.shape[0]):
        lanes = slice(h * HEAD, (h + 1) * HEAD)
        mixer = inside[rows, lanes] + dot(reading[rows, lanes], entering[h], ((1,), (0,)))
        scale = lax.rsqrt(jnp.mean(mixer * mixer, axis=-1, keepdims=True) + 1e-06)
        normed[:, lanes] = (mixer * scale * gain[...]).astype(BF16)
    out[...] = dot(normed[...], matrix[...], ((1,), (0,))).astype(out.dtype)


def final_kernel(kept, received, far, out, sems):
    pieces, rows, _ = out.shape
    copies = []
    for i in range(pieces):
        span = slice(i * rows, (i + 1) * rows)
        out[i] = (kept[span] + received[span].astype(F32)).astype(BF16)
        copies.append(pltpu.make_async_copy(out.at[i], far.at[span], sems.at[i]))
        copies[-1].start()
    for copy in copies:
        copy.wait()


VMEM = 67043328
IN_VMEM = pl.BlockSpec(memory_space=pltpu.VMEM)
IN_HBM = pl.BlockSpec(memory_space=pltpu.HBM)


def call(kernel, name, far, near, outs, flops, scratch=(), left=24 << 20, out_spec=IN_VMEM):
    inputs = (*far, *near)
    moved = sum(a.size * a.dtype.itemsize for a in (*inputs, *outs))
    results = pl.pallas_call(
        kernel,
        name=name,
        out_shape=outs,
        in_specs=[IN_HBM] * len(far) + [IN_VMEM] * len(near),
        out_specs=[out_spec] * len(outs),
        scratch_shapes=list(scratch),
        compiler_params=pltpu.CompilerParams(vmem_limit_bytes=VMEM - left),
        cost_estimate=pl.CostEstimate(flops=flops, bytes_accessed=moved, transcendentals=0),
    )(*inputs)
    return results if len(outs) > 1 else results[0]


def body(
    probe_preactivation,
    retention_preactivation,
    source_entries,
    extra_log_retention,
    retention_slack,
    group_normalizer_gain,
    readout_mapping_matrix,
):
    tokens, channels = probe_preactivation.shape
    heads = channels // HEAD
    positions = lax.axis_size(SP)
    slabs = positions // heads
    rows = HEAD // slabs
    width = readout_mapping_matrix.shape[1]
    slack = retention_slack.reshape(1, channels)
    gain = group_normalizer_gain.reshape(1, HEAD)
    extra = extra_log_retention.T
    flops = 2 * tokens * channels * HEAD
    inputs = (retention_preactivation, extra, slack, source_entries)

    def near(arrays):
        return (
            tuple(pltpu.VMEM(a.shape, a.dtype) for a in arrays),
            pltpu.SemaphoreType.DMA((len(arrays),)),
        )

    message = call(
        lambda *refs: state_kernel(slabs, refs[:4], *refs[4:]),
        "state",
        inputs,
        (),
        [jax.ShapeDtypeStruct((positions, rows // 2 + 1, 2, HEAD), BF16)],
        4 * flops,
        near(inputs),
        0,
    )
    arrived = lax.all_to_all(message, SP, split_axis=0, concat_axis=0, tiled=True)
    inputs = (*inputs, probe_preactivation)
    inside, reading = call(
        lambda *refs: local_kernel(refs[:5], *refs[5:]),
        "local",
        inputs,
        (),
        [jax.ShapeDtypeStruct((tokens, channels), BF16)] * 2,
        6 * flops,
        near(inputs),
        10300000,
    )
    arrived, inside, reading = lax.optimization_barrier((arrived, inside, reading))
    scanned = call(
        functools.partial(scan_kernel, slabs),
        "scan",
        (),
        (arrived,),
        [jax.ShapeDtypeStruct((positions, rows, HEAD), BF16)],
        40 * flops,
        [pltpu.VMEM((HEAD, positions), F32)],
    )
    entering = lax.all_to_all(scanned, SP, split_axis=0, concat_axis=0, tiled=True)
    entering = entering.reshape(heads, HEAD, HEAD)
    half = tokens // lax.axis_size("tp")

    def projected(away, dtype):
        return call(
            functools.partial(output_kernel, away),
            "away" if away else "kept",
            (),
            (inside, reading, entering, gain, readout_mapping_matrix),
            [jax.ShapeDtypeStruct((half, width), dtype)],
            half * channels * width * 2,
            [pltpu.VMEM((half, channels), BF16)],
        )

    received = lax.ppermute(projected(True, BF16), "tp", [(0, 1), (1, 0)])
    pieces = 4
    return call(
        final_kernel,
        "final",
        (),
        (projected(False, F32), received),
        [jax.ShapeDtypeStruct((half, width), BF16)],
        half * width,
        [pltpu.VMEM((pieces, half // pieces, width), BF16), pltpu.SemaphoreType.DMA((pieces,))],
        out_spec=IN_HBM,
    )


def solution(mesh):
    in_specs = (
        P(GRP_SP, "tp"),
        P(GRP_SP, "tp"),
        P(GRP_SP, "tp"),
        P(GRP_SP, "tp"),
        P("tp"),
        P(),
        P("tp", None),
    )
    out_specs = P(GRP_SP_TP, None)
    return jax.shard_map(body, mesh=mesh, in_specs=in_specs, out_specs=out_specs, check_vma=False)
```

```python
import functools

import jax
import jax.numpy as jnp
from jax import lax
from jax.experimental import pallas as pl
from jax.experimental.pallas import tpu as pltpu
from jax.sharding import PartitionSpec as P

SPAN = 128
HEAD = 128
SP = "sp"
GRP_SP = ("grp", "sp")
GRP_SP_TP = ("grp", "sp", "tp")
F32 = jnp.float32
BF16 = jnp.bfloat16


def dot(a, b, contract):
    return lax.dot_general(a, b, (contract, ((), ())), preferred_element_type=F32)


def two_parts(x):
    high = x.astype(BF16)
    return high, (x - high.astype(F32)).astype(BF16)


def summed_rows(selection, x):
    return sum(dot(selection, part, ((1,), (0,))) for part in two_parts(x))


def keyed_and_log_decay(retention, slack, extra):
    keyed = slack * jax.nn.sigmoid(-retention.astype(F32))
    return keyed, jnp.log(1.0 - keyed) + extra


def rows_and_columns(shape):
    return lax.broadcasted_iota(jnp.int32, shape, 0), lax.broadcasted_iota(jnp.int32, shape, 1)


def for_pair(by_token, p):
    return jnp.concatenate(
        [
            jnp.broadcast_to(by_token[:, h : h + 1], (by_token.shape[0], HEAD))
            for h in (2 * p, 2 * p + 1)
        ],
        axis=1,
    )


def copied(pairs, sems):
    copies = [pltpu.make_async_copy(a, b, sems.at[i]) for i, (a, b) in enumerate(pairs)]
    for copy in copies:
        copy.start()
    return copies


def staggered(make, count):
    chains = [make(i) for i in range(count)]
    live = []
    while chains or live:
        if chains:
            live.append(chains.pop(0))
        live = [chain for chain in live if next(chain, live) is None]


def state_kernel(slabs, far, message, near, sems):
    copies = copied(zip(far, near), sems)
    retention, extra, slack, source = near
    tokens, channels = retention.shape
    wide = 2 * HEAD
    rows = HEAD // slabs
    r, c = rows_and_columns((tokens, tokens))
    later = (c > r).astype(BF16)
    for copy in copies[:-1]:
        copy.wait()
    by_token = extra[...].T

    def chain(p):
        lanes = slice(p * wide, (p + 1) * wide)
        keyed, log_decay = keyed_and_log_decay(
            retention[:, lanes], slack[:, lanes], for_pair(by_token, p)
        )
        yield
        ahead = summed_rows(later, log_decay)
        yield
        sent = (keyed * jnp.exp(ahead)).astype(BF16)
        total = ahead[:1] + log_decay[:1]
        parts = jnp.concatenate(two_parts(total), axis=0)
        yield
        if p == 0:
            copies[-1].wait()
        for k in range(2):
            part = slice(k * HEAD, (k + 1) * HEAD)
            h = 2 * p + k
            values = source[:, h * HEAD : (h + 1) * HEAD]
            state = dot(sent[:, part], values, ((0,), (0,)))
            message[h * slabs : (h + 1) * slabs, : rows // 2] = state.astype(BF16).reshape(
                slabs, rows // 2, 2, HEAD
            )
            message[h * slabs : (h + 1) * slabs, rows // 2] = jnp.broadcast_to(
                parts[None, :, part], (slabs, 2, HEAD)
            )

    staggered(chain, channels // wide)


def scan_kernel(slabs, message, entering, by_channel):
    positions, rows, _ = entering.shape
    slab = lax.rem(lax.axis_index(SP), slabs)
    parts = message[:, rows // 2].astype(F32)
    by_channel[...] = jnp.exp(parts[:, 0] + parts[:, 1]).T
    mine = by_channel[pl.ds(pl.multiple_of(slab * rows, rows), rows), :]
    state = jnp.zeros((rows, HEAD), F32)
    for i in range(positions):
        entering[i] = state.astype(BF16)
        if i + 1 < positions:
            state = mine[:, i : i + 1] * state + message[i, : rows // 2].astype(F32).reshape(rows, HEAD)


def local_kernel(far, inside, reading, near, sems):
    copies = copied(zip(far, near), sems)
    retention, extra, slack, source, probe = near
    tokens, channels = retention.shape
    wide = 2 * HEAD
    r, c = rows_and_columns((tokens, tokens))
    within = ((c <= r) & (r // SPAN == c // SPAN)).astype(BF16)
    r, c = rows_and_columns((SPAN, SPAN))
    upto = c <= r
    for copy in copies:
        copy.wait()
    by_token = extra[...].T

    def chain(p):
        lanes = slice(p * wide, (p + 1) * wide)
        keyed, log_decay = keyed_and_log_decay(
            retention[:, lanes], slack[:, lanes], for_pair(by_token, p)
        )
        yield
        running = summed_rows(within, log_decay)
        yield
        raised = jax.nn.silu(probe[:, lanes].astype(F32)) * jnp.exp(running)
        lifted = raised.astype(BF16)
        lowered = (keyed * jnp.exp(-running)).astype(BF16)
        yield
        decayed, before = None, [None, None]
        for b in range(tokens // SPAN):
            span = slice(b * SPAN, (b + 1) * SPAN)
            last = running[(b + 1) * SPAN - 1 : (b + 1) * SPAN]
            if b == 0:
                reading[span, lanes] = lifted[span]
            else:
                reading[span, lanes] = (raised[span] * jnp.exp(decayed)).astype(BF16)
            more = (b + 1) * SPAN < tokens
            if more:
                sent = (keyed[span] * jnp.exp(last - running[span])).astype(BF16)
                decayed = last if b == 0 else decayed + last
            weights = []
            for k in range(2):
                part = slice(k * HEAD, (k + 1) * HEAD)
                scores = dot(lifted[span, part], lowered[span, part], ((1,), (1,)))
                weights.append(jnp.where(upto, scores, 0.0).astype(BF16))
            yield
            for k in range(2):
                part = slice(k * HEAD, (k + 1) * HEAD)
                columns = slice(p * wide + k * HEAD, p * wide + (k + 1) * HEAD)
                values = source[span, columns]
                left, right = weights[k], values
                if b > 0:
                    left = jnp.concatenate([left, lifted[span, part]], axis=1)
                    right = jnp.concatenate([right, before[k].astype(BF16)], axis=0)
                inside[span, columns] = dot(left, right, ((1,), (0,))).astype(BF16)
                if more:
                    added = dot(sent[:, part], values, ((0,), (0,)))
                    if b > 0:
                        added = jnp.exp(last[:, part]).reshape(HEAD, 1) * before[k] + added
                    before[k] = added
            yield

    staggered(chain, channels // wide)


def output_kernel(away, inside, reading, entering, gain, matrix, out, normed):
    tokens = out.shape[0]
    mine = lax.axis_index("tp")
    half = 1 - mine if away else mine
    rows = pl.ds(pl.multiple_of(half * tokens, tokens), tokens)
    for h in range(entering.shape[0]):
        lanes = slice(h * HEAD, (h + 1) * HEAD)
        mixer = inside[rows, lanes] + dot(reading[rows, lanes], entering[h], ((1,), (0,)))
        scale = lax.rsqrt(jnp.mean(mixer * mixer, axis=-1, keepdims=True) + 1e-06)
        normed[:, lanes] = (mixer * scale * gain[...]).astype(BF16)
    out[...] = dot(normed[...], matrix[...], ((1,), (0,))).astype(out.dtype)


def final_kernel(kept, received, far, out, sems):
    pieces, rows, _ = out.shape
    copies = []
    for i in range(pieces):
        span = slice(i * rows, (i + 1) * rows)
        out[i] = (kept[span] + received[span].astype(F32)).astype(BF16)
        copies.append(pltpu.make_async_copy(out.at[i], far.at[span], sems.at[i]))
        copies[-1].start()
    for copy in copies:
        copy.wait()


VMEM = 67043328
IN_VMEM = pl.BlockSpec(memory_space=pltpu.VMEM)
IN_HBM = pl.BlockSpec(memory_space=pltpu.HBM)


def call(kernel, name, far, near, outs, flops, scratch=(), left=24 << 20, out_spec=IN_VMEM):
    inputs = (*far, *near)
    moved = sum(a.size * a.dtype.itemsize for a in (*inputs, *outs))
    results = pl.pallas_call(
        kernel,
        name=name,
        out_shape=outs,
        in_specs=[IN_HBM] * len(far) + [IN_VMEM] * len(near),
        out_specs=[out_spec] * len(outs),
        scratch_shapes=list(scratch),
        compiler_params=pltpu.CompilerParams(vmem_limit_bytes=VMEM - left),
        cost_estimate=pl.CostEstimate(flops=flops, bytes_accessed=moved, transcendentals=0),
    )(*inputs)
    return results if len(outs) > 1 else results[0]


def body(
    probe_preactivation,
    retention_preactivation,
    source_entries,
    extra_log_retention,
    retention_slack,
    group_normalizer_gain,
    readout_mapping_matrix,
):
    tokens, channels = probe_preactivation.shape
    heads = channels // HEAD
    positions = lax.axis_size(SP)
    slabs = positions // heads
    rows = HEAD // slabs
    width = readout_mapping_matrix.shape[1]
    slack = retention_slack.reshape(1, channels)
    gain = group_normalizer_gain.reshape(1, HEAD)
    extra = extra_log_retention.T
    flops = 2 * tokens * channels * HEAD
    inputs = (retention_preactivation, extra, slack, source_entries)

    def near(arrays):
        return (
            tuple(pltpu.VMEM(a.shape, a.dtype) for a in arrays),
            pltpu.SemaphoreType.DMA((len(arrays),)),
        )

    message = call(
        lambda *refs: state_kernel(slabs, refs[:4], *refs[4:]),
        "state",
        inputs,
        (),
        [jax.ShapeDtypeStruct((positions, rows // 2 + 1, 2, HEAD), BF16)],
        4 * flops,
        near(inputs),
        0,
    )
    arrived = lax.all_to_all(message, SP, split_axis=0, concat_axis=0, tiled=True)
    inputs = (*inputs, probe_preactivation)
    inside, reading = call(
        lambda *refs: local_kernel(refs[:5], *refs[5:]),
        "local",
        inputs,
        (),
        [jax.ShapeDtypeStruct((tokens, channels), BF16)] * 2,
        6 * flops,
        near(inputs),
        11600000,
    )
    arrived, inside, reading = lax.optimization_barrier((arrived, inside, reading))
    scanned = call(
        functools.partial(scan_kernel, slabs),
        "scan",
        (),
        (arrived,),
        [jax.ShapeDtypeStruct((positions, rows, HEAD), BF16)],
        40 * flops,
        [pltpu.VMEM((HEAD, positions), F32)],
    )
    entering = lax.all_to_all(scanned, SP, split_axis=0, concat_axis=0, tiled=True)
    entering = entering.reshape(heads, HEAD, HEAD)
    half = tokens // lax.axis_size("tp")

    def projected(away, dtype):
        return call(
            functools.partial(output_kernel, away),
            "away" if away else "kept",
            (),
            (inside, reading, entering, gain, readout_mapping_matrix),
            [jax.ShapeDtypeStruct((half, width), dtype)],
            half * channels * width * 2,
            [pltpu.VMEM((half, channels), BF16)],
        )

    received = lax.ppermute(projected(True, BF16), "tp", [(0, 1), (1, 0)])
    pieces = 4
    return call(
        final_kernel,
        "final",
        (),
        (projected(False, F32), received),
        [jax.ShapeDtypeStruct((half, width), BF16)],
        half * width,
        [pltpu.VMEM((pieces, half // pieces, width), BF16), pltpu.SemaphoreType.DMA((pieces,))],
        out_spec=IN_HBM,
    )


def solution(mesh):
    in_specs = (
        P(GRP_SP, "tp"),
        P(GRP_SP, "tp"),
        P(GRP_SP, "tp"),
        P(GRP_SP, "tp"),
        P("tp"),
        P(),
        P("tp", None),
    )
    out_specs = P(GRP_SP_TP, None)
    return jax.shard_map(body, mesh=mesh, in_specs=in_specs, out_specs=out_specs, check_vma=False)
```

```python
import functools

import jax
import jax.numpy as jnp
from jax import lax
from jax.experimental import pallas as pl
from jax.experimental.pallas import tpu as pltpu
from jax.sharding import PartitionSpec as P

SPAN = 128
HEAD = 128
SP = "sp"
GRP_SP = ("grp", "sp")
GRP_SP_TP = ("grp", "sp", "tp")
F32 = jnp.float32
BF16 = jnp.bfloat16


def dot(a, b, contract):
    return lax.dot_general(a, b, (contract, ((), ())), preferred_element_type=F32)


def two_parts(x):
    high = x.astype(BF16)
    return high, (x - high.astype(F32)).astype(BF16)


def summed_rows(selection, x):
    return sum(dot(selection, part, ((1,), (0,))) for part in two_parts(x))


def keyed_and_log_decay(retention, slack, extra):
    keyed = slack * jax.nn.sigmoid(-retention.astype(F32))
    return keyed, jnp.log(1.0 - keyed) + extra


def rows_and_columns(shape):
    return lax.broadcasted_iota(jnp.int32, shape, 0), lax.broadcasted_iota(jnp.int32, shape, 1)


def for_pair(by_token, p):
    return jnp.concatenate(
        [
            jnp.broadcast_to(by_token[:, h : h + 1], (by_token.shape[0], HEAD))
            for h in (2 * p, 2 * p + 1)
        ],
        axis=1,
    )


def copied(pairs, sems):
    copies = [pltpu.make_async_copy(a, b, sems.at[i]) for i, (a, b) in enumerate(pairs)]
    for copy in copies:
        copy.start()
    return copies


def staggered(make, count):
    chains = [make(i) for i in range(count)]
    live = []
    while chains or live:
        if chains:
            live.append(chains.pop(0))
        live = [chain for chain in live if next(chain, live) is None]


def state_kernel(slabs, far, message, near, sems):
    copies = copied(zip(far, near), sems)
    retention, extra, slack, source = near
    tokens, channels = retention.shape
    wide = 2 * HEAD
    rows = HEAD // slabs
    r, c = rows_and_columns((tokens, tokens))
    later = (c > r).astype(BF16)
    for copy in copies[:-1]:
        copy.wait()
    by_token = extra[...].T

    def chain(p):
        lanes = slice(p * wide, (p + 1) * wide)
        keyed, log_decay = keyed_and_log_decay(
            retention[:, lanes], slack[:, lanes], for_pair(by_token, p)
        )
        yield
        ahead = summed_rows(later, log_decay)
        yield
        sent = (keyed * jnp.exp(ahead)).astype(BF16)
        total = ahead[:1] + log_decay[:1]
        parts = jnp.concatenate(two_parts(total), axis=0)
        yield
        if p == 0:
            copies[-1].wait()
        for k in range(2):
            part = slice(k * HEAD, (k + 1) * HEAD)
            h = 2 * p + k
            values = source[:, h * HEAD : (h + 1) * HEAD]
            state = dot(sent[:, part], values, ((0,), (0,)))
            message[h * slabs : (h + 1) * slabs, : rows // 2] = state.astype(BF16).reshape(
                slabs, rows // 2, 2, HEAD
            )
            message[h * slabs : (h + 1) * slabs, rows // 2] = jnp.broadcast_to(
                parts[None, :, part], (slabs, 2, HEAD)
            )

    staggered(chain, channels // wide)


def scan_kernel(slabs, message, entering, by_channel):
    positions, rows, _ = entering.shape
    slab = lax.rem(lax.axis_index(SP), slabs)
    parts = message[:, rows // 2].astype(F32)
    by_channel[...] = jnp.exp(parts[:, 0] + parts[:, 1]).T
    mine = by_channel[pl.ds(pl.multiple_of(slab * rows, rows), rows), :]
    state = jnp.zeros((rows, HEAD), F32)
    for i in range(positions):
        entering[i] = state.astype(BF16)
        if i + 1 < positions:
            state = mine[:, i : i + 1] * state + message[i, : rows // 2].astype(F32).reshape(rows, HEAD)


def local_kernel(far, inside, reading, near, sems):
    copies = copied(zip(far, near), sems)
    retention, extra, slack, source, probe = near
    tokens, channels = retention.shape
    wide = 2 * HEAD
    r, c = rows_and_columns((tokens, tokens))
    within = ((c <= r) & (r // SPAN == c // SPAN)).astype(BF16)
    r, c = rows_and_columns((SPAN, SPAN))
    upto = c <= r
    for copy in copies:
        copy.wait()
    by_token = extra[...].T

    def chain(p):
        lanes = slice(p * wide, (p + 1) * wide)
        keyed, log_decay = keyed_and_log_decay(
            retention[:, lanes], slack[:, lanes], for_pair(by_token, p)
        )
        yield
        running = summed_rows(within, log_decay)
        yield
        raised = jax.nn.silu(probe[:, lanes].astype(F32)) * jnp.exp(running)
        lifted = raised.astype(BF16)
        lowered = (keyed * jnp.exp(-running)).astype(BF16)
        yield
        decayed, before = None, [None, None]
        for b in range(tokens // SPAN):
            span = slice(b * SPAN, (b + 1) * SPAN)
            last = running[(b + 1) * SPAN - 1 : (b + 1) * SPAN]
            if b == 0:
                reading[span, lanes] = lifted[span]
            else:
                reading[span, lanes] = (raised[span] * jnp.exp(decayed)).astype(BF16)
            more = (b + 1) * SPAN < tokens
            if more:
                sent = (keyed[span] * jnp.exp(last - running[span])).astype(BF16)
                decayed = last if b == 0 else decayed + last
            weights = []
            for k in range(2):
                part = slice(k * HEAD, (k + 1) * HEAD)
                scores = dot(lifted[span, part], lowered[span, part], ((1,), (1,)))
                weights.append(jnp.where(upto, scores, 0.0).astype(BF16))
            yield
            for k in range(2):
                part = slice(k * HEAD, (k + 1) * HEAD)
                columns = slice(p * wide + k * HEAD, p * wide + (k + 1) * HEAD)
                values = source[span, columns]
                left, right = weights[k], values
                if b > 0:
                    left = jnp.concatenate([left, lifted[span, part]], axis=1)
                    right = jnp.concatenate([right, before[k].astype(BF16)], axis=0)
                inside[span, columns] = dot(left, right, ((1,), (0,))).astype(BF16)
                if more:
                    added = dot(sent[:, part], values, ((0,), (0,)))
                    if b > 0:
                        added = jnp.exp(last[:, part]).reshape(HEAD, 1) * before[k] + added
                    before[k] = added
            yield

    staggered(chain, channels // wide)


def output_kernel(away, inside, reading, entering, gain, matrix, out, normed):
    tokens = out.shape[0]
    mine = lax.axis_index("tp")
    half = 1 - mine if away else mine
    rows = pl.ds(pl.multiple_of(half * tokens, tokens), tokens)

    def chain(h):
        lanes = slice(h * HEAD, (h + 1) * HEAD)
        read = dot(reading[rows, lanes], entering[h], ((1,), (0,)))
        yield
        mixer = inside[rows, lanes] + read
        scale = lax.rsqrt(jnp.mean(mixer * mixer, axis=-1, keepdims=True) + 1e-06)
        yield
        normed[:, lanes] = (mixer * scale * gain[...]).astype(BF16)

    staggered(chain, entering.shape[0])
    out[...] = dot(normed[...], matrix[...], ((1,), (0,))).astype(out.dtype)


def final_kernel(kept, received, far, out, sems):
    pieces, rows, _ = out.shape
    copies = []
    for i in range(pieces):
        span = slice(i * rows, (i + 1) * rows)
        out[i] = (kept[span] + received[span].astype(F32)).astype(BF16)
        copies.append(pltpu.make_async_copy(out.at[i], far.at[span], sems.at[i]))
        copies[-1].start()
    for copy in copies:
        copy.wait()


VMEM = 67043328
IN_VMEM = pl.BlockSpec(memory_space=pltpu.VMEM)
IN_HBM = pl.BlockSpec(memory_space=pltpu.HBM)


def call(kernel, name, far, near, outs, flops, scratch=(), left=24 << 20, out_spec=IN_VMEM):
    inputs = (*far, *near)
    moved = sum(a.size * a.dtype.itemsize for a in (*inputs, *outs))
    results = pl.pallas_call(
        kernel,
        name=name,
        out_shape=outs,
        in_specs=[IN_HBM] * len(far) + [IN_VMEM] * len(near),
        out_specs=[out_spec] * len(outs),
        scratch_shapes=list(scratch),
        compiler_params=pltpu.CompilerParams(vmem_limit_bytes=VMEM - left),
        cost_estimate=pl.CostEstimate(flops=flops, bytes_accessed=moved, transcendentals=0),
    )(*inputs)
    return results if len(outs) > 1 else results[0]


def body(
    probe_preactivation,
    retention_preactivation,
    source_entries,
    extra_log_retention,
    retention_slack,
    group_normalizer_gain,
    readout_mapping_matrix,
):
    tokens, channels = probe_preactivation.shape
    heads = channels // HEAD
    positions = lax.axis_size(SP)
    slabs = positions // heads
    rows = HEAD // slabs
    width = readout_mapping_matrix.shape[1]
    slack = retention_slack.reshape(1, channels)
    gain = group_normalizer_gain.reshape(1, HEAD)
    extra = extra_log_retention.T
    flops = 2 * tokens * channels * HEAD
    inputs = (retention_preactivation, extra, slack, source_entries)

    def near(arrays):
        return (
            tuple(pltpu.VMEM(a.shape, a.dtype) for a in arrays),
            pltpu.SemaphoreType.DMA((len(arrays),)),
        )

    message = call(
        lambda *refs: state_kernel(slabs, refs[:4], *refs[4:]),
        "state",
        inputs,
        (),
        [jax.ShapeDtypeStruct((positions, rows // 2 + 1, 2, HEAD), BF16)],
        4 * flops,
        near(inputs),
        0,
    )
    arrived = lax.all_to_all(message, SP, split_axis=0, concat_axis=0, tiled=True)
    inputs = (*inputs, probe_preactivation)
    inside, reading = call(
        lambda *refs: local_kernel(refs[:5], *refs[5:]),
        "local",
        inputs,
        (),
        [jax.ShapeDtypeStruct((tokens, channels), BF16)] * 2,
        6 * flops,
        near(inputs),
        10300000,
    )
    arrived, inside, reading = lax.optimization_barrier((arrived, inside, reading))
    scanned = call(
        functools.partial(scan_kernel, slabs),
        "scan",
        (),
        (arrived,),
        [jax.ShapeDtypeStruct((positions, rows, HEAD), BF16)],
        40 * flops,
        [pltpu.VMEM((HEAD, positions), F32)],
    )
    entering = lax.all_to_all(scanned, SP, split_axis=0, concat_axis=0, tiled=True)
    entering = entering.reshape(heads, HEAD, HEAD)
    half = tokens // lax.axis_size("tp")

    def projected(away, dtype):
        return call(
            functools.partial(output_kernel, away),
            "away" if away else "kept",
            (),
            (inside, reading, entering, gain, readout_mapping_matrix),
            [jax.ShapeDtypeStruct((half, width), dtype)],
            half * channels * width * 2,
            [pltpu.VMEM((half, channels), BF16)],
        )

    received = lax.ppermute(projected(True, BF16), "tp", [(0, 1), (1, 0)])
    pieces = 4
    return call(
        final_kernel,
        "final",
        (),
        (projected(False, F32), received),
        [jax.ShapeDtypeStruct((half, width), BF16)],
        half * width,
        [pltpu.VMEM((pieces, half // pieces, width), BF16), pltpu.SemaphoreType.DMA((pieces,))],
        out_spec=IN_HBM,
    )


def solution(mesh):
    in_specs = (
        P(GRP_SP, "tp"),
        P(GRP_SP, "tp"),
        P(GRP_SP, "tp"),
        P(GRP_SP, "tp"),
        P("tp"),
        P(),
        P("tp", None),
    )
    out_specs = P(GRP_SP_TP, None)
    return jax.shard_map(body, mesh=mesh, in_specs=in_specs, out_specs=out_specs, check_vma=False)
```
